32 devices in a mesh: grp: 2 (over y), ep: 8 (over z, core), tp: 2 (over x).
Axes of the slice: x: 2, y: 2, z: 4, core: 2. Of those that a mesh axis runs over, the one named last changes fastest.
Arguments:
- resid_in: bfloat16 [176, 2048], P(('grp', 'ep')), parts along dimension 0, may hold values from -6 to 6
- norm_attn: float32 [2048], replicated, may hold values from 0.1 to 1.9
- norm_moe: float32 [2048], replicated, may hold values from 0.1 to 1.9
- w_query: bfloat16 [2048, 1024], P('ep', 'tp'), may hold values from -0.125 to 0.125
- w_key: bfloat16 [2048, 256], P('ep', 'tp'), may hold values from -0.125 to 0.125
- w_value: bfloat16 [2048, 256], P('ep', 'tp'), may hold values from -0.125 to 0.125
- head_offset: float32 [16], P('tp'), may hold values from 1.5 to 9.5
- kv_cache: bfloat16 [176, 1024, 4, 128], P(('grp', 'ep'), None, 'tp'), parts along dimension 0, may hold values from -6 to 6
- lengths: int32 [176], P(('grp', 'ep')), parts along dimension 0, may hold values from 128 to 1024, as said below
- w_output: bfloat16 [1024, 2048], P('tp', 'ep'), may hold values from -0.375 to 0.375
- routes: int32 [176, 4], P(('grp', 'ep')), parts along dimension 0, may hold values from 0 to 7, all different within a row; in each aligned block of 11 rows (0 to 10, 11 to 21, ...) at most 7 rows name the same one
- route_weights: float32 [176, 4], P(('grp', 'ep')), parts along dimension 0, may hold values from 0.2 to 1
- gate_experts: bfloat16 [8, 2048, 512], P('ep', None, 'tp'), may hold values from -0.125 to 0.125
- up_experts: bfloat16 [8, 2048, 512], P('ep', None, 'tp'), may hold values from -0.125 to 0.125
- down_experts: bfloat16 [8, 512, 2048], P('ep', 'tp'), may hold values from -0.25 to 0.25
- gate_shared: bfloat16 [2048, 512], P('ep', 'tp'), may hold values from -0.125 to 0.125
- up_shared: bfloat16 [2048, 512], P('ep', 'tp'), may hold values from -0.125 to 0.125
- down_shared: bfloat16 [512, 2048], P('tp', 'ep'), may hold values from -0.25 to 0.25
Outputs:
- layer_out: bfloat16 [176, 2048], P(('grp', 'ep'), 'tp'), parts along dimension 0
- new_rows: bfloat16 [176, 4, 128], P(('grp', 'ep'), 'tp'), parts along dimension 0
The draws below stay inside these ranges and needn't reach their ends.
There are 2 independent parts, one for each index of `grp`. The reference program is written for one: setup_inputs(seed, part) draws one part's arguments, and reference() takes and returns one part's arrays. A program takes and returns all parts, laid end to end along the dimension named above; an argument that names none is the same for every part. Nothing has to cross between parts.
Inputs may be any that keep to these rules, and one draw needn't show every extreme that they name: `routes`: among the rows of one device no expert is named more than 7 times, and in every draw some expert is named exactly 7 times by one device's rows; a row names 4 different experts. Sequence b's new token follows cache positions 0 to lengths[b] - 1; the other positions are not read.
All inputs are finite; a program needn't handle non-finite values.
Results may differ from the reference program's by a relative error of at most 0.015.
Values may be sent and summed in bfloat16 or wider, within the bound.
A program may use at most 64 MiB of HBM per device.

```python
import math
import jax
import jax.numpy as jnp
import numpy as np
from jax import lax

D = 2048
HEADS = 16
KV_HEADS = 4
HEAD = 64
FE = 512
FS = 512
TOPK = 4
LEN = 1024
SEQ_DEV = 11
EXPERTS = 8
TOKENS = 88
CAP = 7
N_EP = 8
N_TP = 2


def draw_head_offset(key, part):
    key_one, key_two = jax.random.split(key)
    order = jax.random.permutation(key_two, HEADS)
    fast_rate = jax.random.uniform(key_one, (HEADS,), jnp.float32, 1.5, 3.0)
    slow_rate = jax.random.uniform(jax.random.fold_in(key_one, 7), (HEADS,), jnp.float32, 6.5, 9.0)
    return jnp.where(order < HEADS // 2, fast_rate, slow_rate)


def draw_lengths(key, part):
    key_one, key_two = jax.random.split(key)
    drawn = jax.random.randint(key_one, (TOKENS,), LEN // 8, LEN + 1, dtype=jnp.int32)
    chosen = jax.random.randint(key_two, (), 0, TOKENS, dtype=jnp.int32)
    drawn = drawn.at[chosen].set(LEN)
    return drawn.at[(chosen + 1) % TOKENS].set(LEN // 8)


def level_of(stream_key, shape, cuts, least, high):
    def one(axis_at, blocks):
        steps = jax.random.uniform(jax.random.fold_in(jax.random.fold_in(stream_key, 6), axis_at), (blocks,), jnp.float32, least / len(cuts), high / len(cuts))
        return jnp.repeat(jnp.exp(steps), shape[axis_at] // blocks).reshape((-1,) + (1,) * (len(shape) - axis_at - 1))

    factor_of = one(*cuts[0])
    for cut in cuts[1:]:
        factor_of = factor_of * one(*cut)
    return factor_of


def routed_block(rng, own, number, rows, amount, top, most, lean):
    order = jax.random.permutation(rng, amount)
    crowded, ordinary = portions_of(amount, rows * top, most, lean, True), portions_of(amount, rows * top, most, lean, False)
    places = jnp.arange(amount)

    def named(sizes, turn):
        used = int((sizes > 0).sum())
        fixed = max(1, used // 4)
        moved = fixed + (places - fixed + turn * (used - fixed)) % max(1, amount - fixed)
        return jnp.zeros((amount,), jnp.int32).at[order[jnp.where(places < fixed, places, moved)]].set(jnp.asarray(sizes, jnp.int32))

    sizes = jnp.where(number % 4 == 0, named(crowded, number // 4), named(ordinary, number - number // 4 - 1))
    mixed = jax.random.permutation(jax.random.fold_in(own, 3), amount)
    giver, sink = mixed[0:amount // 2 * 2:2], mixed[1:amount // 2 * 2:2]
    margin = jnp.minimum(sizes[giver] - 1, most - sizes[sink]) // 2
    margin = jnp.where((giver == order[0]) | (sink == order[0]) | (sizes[sink] == 0), 0, jnp.maximum(margin, 0))
    moved = jax.random.randint(jax.random.fold_in(own, 4), (amount // 2,), 0, 1 << 20) % (margin + 1)
    sizes = sizes.at[giver].add(-moved).at[sink].add(moved)
    labels = jnp.searchsorted(jnp.cumsum(sizes), jnp.arange(rows * top), side="right").astype(jnp.int32)
    grid = labels.reshape(top, rows).T
    grid = grid[jax.random.permutation(jax.random.fold_in(own, 1), rows)]
    turn = jax.random.randint(jax.random.fold_in(own, 2), (rows, 1), 0, top)
    return jnp.take_along_axis(grid, (jnp.arange(top)[None, :] + turn) % top, axis=1)


def portions_of(count, total, most, skew, full):
    loads = [(1 << 20) // math.isqrt(grade ** skew) + 1 for grade in range(1, count + 1)]
    largest = most if full else min(most, max(-(-total // count), total * loads[0] // sum(loads)))
    least = 1 if total - largest >= count - 1 else 0
    given, rest = [largest] + [least] * (count - 1), total - largest - least * (count - 1)
    while rest > 0:
        movable = [i for i in range(1, count) if given[i] < largest] or [i for i in range(1, count) if given[i] < most]
        pool, budget = sum([loads[i] for i in movable]), rest
        for i in movable:
            addition = min(most - given[i], max(1, budget * loads[i] // pool), rest)
            given[i] = given[i] + addition
            rest = rest - addition
    return np.array(given)


def noise(key, dims, deviation, reach, cuts=(), kind=jnp.bfloat16):
    values = deviation * jax.random.normal(key, dims, jnp.float32)
    if cuts:
        values = values * level_of(key, dims, cuts, -0.22, 0.18)
    return jnp.clip(values, -reach, reach).astype(kind)


def setup_inputs(seed: int = 0, part: int = 0) -> dict:
    splits = jax.random.split(jax.random.key(seed), 19)
    part_splits = jax.random.split(jax.random.fold_in(splits[18], part), 19)
    resid_in = noise(part_splits[0], (TOKENS, D), 1.0, 6.0, ((0, 8),))
    norm_attn = jnp.clip(1.0 + 0.18 * jax.random.normal(splits[1], (D,), jnp.float32), 0.1, 1.9)
    norm_moe = jnp.clip(1.0 + 0.18 * jax.random.normal(splits[2], (D,), jnp.float32), 0.1, 1.9)
    w_query = noise(splits[3], (D, HEADS * HEAD), D ** -0.5, 0.125, ((0, 8), (1, 2)))
    w_key = noise(splits[4], (D, KV_HEADS * HEAD), D ** -0.5, 0.125, ((0, 8), (1, 2)))
    w_value = noise(splits[5], (D, KV_HEADS * HEAD), D ** -0.5, 0.125, ((0, 8), (1, 2)))
    head_offset = draw_head_offset(jax.random.fold_in(splits[18], 71), part)
    kv_cache = noise(part_splits[7], (TOKENS, LEN, KV_HEADS, 2 * HEAD), 1.0, 6.0, ((0, 8), (2, 2)))
    lengths = draw_lengths(jax.random.fold_in(jax.random.fold_in(splits[18], part), 71), part)
    w_output = noise(splits[9], (HEADS * HEAD, D), (HEADS * HEAD // 4) ** -0.5, 0.375, ((0, 2), (1, 8)))
    routes_keys = jax.random.split(jax.random.fold_in(part_splits[10], 1), TOKENS // SEQ_DEV)
    routes_turns = jax.random.permutation(jax.random.fold_in(part_splits[10], 3), TOKENS // SEQ_DEV)
    routes = jax.vmap(lambda own, number: routed_block(jax.random.fold_in(part_splits[10], 2), own, number, SEQ_DEV, EXPERTS, TOPK, CAP, 1))(routes_keys, routes_turns).reshape((TOKENS, TOPK))
    route_weights = jnp.clip(0.2 + 0.8 * jax.random.uniform(part_splits[11], (TOKENS, TOPK), jnp.float32) ** level_of(part_splits[11], (TOKENS, TOPK), ((0, 8),), -0.2, 0.2), 0.2, 1.0)
    gate_experts = noise(splits[12], (EXPERTS, D, FE), D ** -0.5, 0.125, ((0, 8), (2, 2)))
    up_experts = noise(splits[13], (EXPERTS, D, FE), D ** -0.5, 0.125, ((0, 8), (2, 2)))
    down_experts = noise(splits[14], (EXPERTS, FE, D), FE ** -0.5, 0.25, ((0, 8), (1, 2)))
    gate_shared = noise(splits[15], (D, FS), D ** -0.5, 0.125, ((0, 8), (1, 2)))
    up_shared = noise(splits[16], (D, FS), D ** -0.5, 0.125, ((0, 8), (1, 2)))
    down_shared = noise(splits[17], (FS, D), FS ** -0.5, 0.25, ((0, 2), (1, 8)))
    return {"resid_in": resid_in, "norm_attn": norm_attn, "norm_moe": norm_moe, "w_query": w_query, "w_key": w_key, "w_value": w_value, "head_offset": head_offset, "kv_cache": kv_cache, "lengths": lengths, "w_output": w_output, "routes": routes, "route_weights": route_weights, "gate_experts": gate_experts, "up_experts": up_experts, "down_experts": down_experts, "gate_shared": gate_shared, "up_shared": up_shared, "down_shared": down_shared}


EPS = 1e-06

def rms_scale(row_block, gain):
    rows_wide = row_block.astype(jnp.float32)
    inverse = lax.rsqrt(lax.optimization_barrier(jnp.mean(rows_wide * rows_wide, axis=-1, keepdims=True)) + EPS)
    return rows_wide * inverse * gain.astype(jnp.float32)

def grouped_sum(left_rows, right_rows, groups):
    group_width = left_rows.shape[1] // groups
    running = jnp.zeros((left_rows.shape[0], right_rows.shape[1]), jnp.float32)
    for group_idx in range(groups):
        low = group_idx * group_width
        partial_prod = jnp.dot(left_rows[:, low:low + group_width], right_rows[low:low + group_width], preferred_element_type=jnp.float32)
        rounded = lax.optimization_barrier(partial_prod.astype(jnp.bfloat16))
        running = running + rounded.astype(jnp.float32)
    return running

def reference(resid_in, norm_attn, norm_moe, w_query, w_key, w_value, head_offset, kv_cache, lengths, w_output, routes, route_weights, gate_experts, up_experts, down_experts, gate_shared, up_shared, down_shared):
    seq_count = resid_in.shape[0]
    normed = rms_scale(resid_in, norm_attn).astype(jnp.bfloat16)
    query = jnp.dot(normed, w_query, preferred_element_type=jnp.float32).astype(jnp.bfloat16)
    key_new = jnp.dot(normed, w_key, preferred_element_type=jnp.float32).astype(jnp.bfloat16)
    value_new = jnp.dot(normed, w_value, preferred_element_type=jnp.float32).astype(jnp.bfloat16)
    new_rows = jnp.concatenate([key_new.reshape(seq_count, KV_HEADS, HEAD), value_new.reshape(seq_count, KV_HEADS, HEAD)], axis=2)
    offsets = head_offset.astype(jnp.float32).reshape(KV_HEADS, HEADS // KV_HEADS, 1)

    def stick_one(inputs):
        query_row, cache_rows, length_one = inputs
        query_heads = query_row.astype(jnp.float32).reshape(KV_HEADS, HEADS // KV_HEADS, HEAD)
        key_rows = cache_rows[:, :, :HEAD].astype(jnp.float32)
        value_rows = cache_rows[:, :, HEAD:].astype(jnp.float32)
        scores = jnp.einsum('kgd,lkd->kgl', query_heads, key_rows) * HEAD ** (-0.5) - offsets
        alive_mask = (jnp.arange(LEN, dtype=jnp.int32) < length_one)[None, None, :]
        remain = jnp.where(alive_mask, jax.nn.log_sigmoid(-scores), 0.0)
        suffix = lax.cumsum(remain, axis=2, reverse=True) - remain
        stick = jnp.where(alive_mask, jnp.exp(jax.nn.log_sigmoid(scores) + suffix), 0.0)
        stick = lax.optimization_barrier(stick.astype(jnp.bfloat16))
        mixed_out = jnp.einsum('kgl,lkd->kgd', stick.astype(jnp.float32), value_rows)
        return mixed_out.reshape(HEADS * HEAD).astype(jnp.bfloat16)
    attended = lax.map(stick_one, (query, kv_cache, lengths))
    attn_sum = grouped_sum(attended, w_output, N_TP)
    resid_mid = (resid_in.astype(jnp.float32) + attn_sum).astype(jnp.bfloat16)
    normed_moe = rms_scale(resid_mid, norm_moe).astype(jnp.bfloat16)
    gate_s = jnp.dot(normed_moe, gate_shared, preferred_element_type=jnp.float32)
    up_s = jnp.dot(normed_moe, up_shared, preferred_element_type=jnp.float32)
    hidden_shared = (jax.nn.silu(gate_s) * up_s).astype(jnp.bfloat16)
    shared_out = grouped_sum(hidden_shared, down_shared, N_TP)
    flat_routes = routes.reshape(-1)
    flat_weights = jnp.concatenate([route_weights.reshape(-1).astype(jnp.float32), jnp.zeros((1,), jnp.float32)])
    padded_rows = jnp.concatenate([normed_moe, jnp.zeros((1, D), jnp.bfloat16)], axis=0)
    most_rows = CAP * N_EP

    def expert_term(expert_id):
        picked = jnp.nonzero(flat_routes == expert_id, size=most_rows, fill_value=flat_routes.shape[0])[0].astype(jnp.int32)
        token_ids = picked // TOPK
        rows_in = padded_rows[token_ids]
        gate_h = jnp.dot(rows_in, gate_experts[expert_id], preferred_element_type=jnp.float32)
        up_h = jnp.dot(rows_in, up_experts[expert_id], preferred_element_type=jnp.float32)
        hidden_e = (jax.nn.silu(gate_h) * up_h).astype(jnp.bfloat16)
        expert_out = lax.optimization_barrier(grouped_sum(hidden_e, down_experts[expert_id], N_TP).astype(jnp.bfloat16))
        return (expert_out.astype(jnp.float32) * flat_weights[picked][:, None], token_ids)
    terms, token_all = lax.map(expert_term, jnp.arange(EXPERTS, dtype=jnp.int32))
    routed = jnp.zeros((seq_count + 1, D), jnp.float32).at[token_all.reshape(-1)].add(terms.reshape(-1, D))
    layer_out = (resid_mid.astype(jnp.float32) + shared_out + routed[:seq_count]).astype(jnp.bfloat16)
    return (layer_out, new_rows)
```

```python
import functools

import jax
import jax.numpy as jnp
from jax import lax
from jax.experimental import pallas as pl
from jax.experimental.pallas import tpu as pltpu
from jax.sharding import PartitionSpec as P

HEAD = 64
TOPK = 4


EPS = 1e-06


def rms_scale(row_block, gain):
    rows_wide = row_block.astype(jnp.float32)
    inverse = lax.rsqrt(jnp.mean(rows_wide * rows_wide, axis=-1, keepdims=True) + EPS)
    return rows_wide * inverse * gain


def stick_read(query, kv_cache, lengths, offsets):
    seq_count = query.shape[0]
    kv_local = kv_cache.shape[2]
    head_local = offsets.shape[0]
    per_group = head_local // kv_local
    cache_len = kv_cache.shape[1]
    grouped = query.reshape(seq_count, kv_local, per_group, HEAD)
    key_rows = kv_cache[:, :, :, :HEAD]
    value_rows = kv_cache[:, :, :, HEAD:]
    scores = jnp.einsum("skgd,slkd->skgl", grouped, key_rows, preferred_element_type=jnp.float32)
    scores = scores * HEAD ** (-0.5) - offsets.reshape(1, kv_local, per_group, 1)
    positions = lax.broadcasted_iota(jnp.int32, (seq_count, cache_len), 1)
    alive_mask = (positions < lengths[:, None])[:, None, None, :]
    remain = jnp.where(alive_mask, jax.nn.log_sigmoid(-scores), 0.0)
    suffix = lax.cumsum(remain, axis=3, reverse=True) - remain
    stick = jnp.where(alive_mask, jnp.exp(jax.nn.log_sigmoid(scores) + suffix), 0.0).astype(
        jnp.bfloat16
    )
    mixed_out = jnp.einsum("skgl,slkd->skgd", stick, value_rows, preferred_element_type=jnp.float32)
    return mixed_out.reshape(seq_count, head_local * HEAD).astype(jnp.bfloat16)


def on_device(
    resid_in,
    norm_attn,
    norm_moe,
    w_query,
    w_key,
    w_value,
    head_offset,
    kv_cache,
    lengths,
    w_output,
    routes,
    route_weights,
    gate_experts,
    up_experts,
    down_experts,
    gate_shared,
    up_shared,
    down_shared,
):
    tok_count = resid_in.shape[0]
    n_ep = lax.axis_size("ep")
    normed = rms_scale(resid_in, norm_attn).astype(jnp.bfloat16)
    k_cols = w_key.shape[1]
    pieces = (
        lax.all_gather(w_query, "ep", axis=0, tiled=True),
        lax.all_gather(w_key, "ep", axis=0, tiled=True),
        lax.all_gather(w_value, "ep", axis=0, tiled=True),
    )
    sliced = normed
    query_f, key_f, value_f = tuple(
        (
            jnp.dot(sliced, weight_piece, preferred_element_type=jnp.float32)
            for weight_piece in pieces
        )
    )
    query = query_f.astype(jnp.bfloat16)
    kv_local = k_cols // HEAD
    key_new = key_f.astype(jnp.bfloat16).reshape(tok_count, kv_local, HEAD)
    value_new = value_f.astype(jnp.bfloat16).reshape(tok_count, kv_local, HEAD)
    new_rows = jnp.concatenate([key_new, value_new], axis=2)
    attended = stick_read(query, kv_cache, lengths, head_offset)
    attn_part = jnp.dot(
        attended,
        lax.all_gather(w_output, "ep", axis=1, tiled=True),
        preferred_element_type=jnp.float32,
    ).astype(jnp.bfloat16)
    attn_sum = lax.psum(attn_part, "tp").astype(jnp.float32)
    resid_mid = (resid_in.astype(jnp.float32) + attn_sum).astype(jnp.bfloat16)
    normed_moe = rms_scale(resid_mid, norm_moe).astype(jnp.bfloat16)
    pieces = (
        lax.all_gather(gate_shared, "ep", axis=0, tiled=True),
        lax.all_gather(up_shared, "ep", axis=0, tiled=True),
    )
    sliced = normed_moe
    gate_s = jnp.dot(sliced, pieces[0], preferred_element_type=jnp.float32)
    up_s = jnp.dot(sliced, pieces[1], preferred_element_type=jnp.float32)
    hidden_shared = (jax.nn.silu(gate_s) * up_s).astype(jnp.bfloat16)
    shared_part = jnp.dot(
        hidden_shared,
        lax.all_gather(down_shared, "ep", axis=1, tiled=True),
        preferred_element_type=jnp.float32,
    ).astype(jnp.bfloat16)
    shared_out = lax.psum_scatter(shared_part, "tp", scatter_dimension=1, tiled=True).astype(
        jnp.float32
    )
    local_experts = gate_experts.shape[0]
    experts_all = local_experts * n_ep
    capacity = min(tok_count, tok_count * TOPK // experts_all + 2)
    flat_routes = routes.reshape(-1)
    expert_ids = lax.broadcasted_iota(jnp.int32, (1, experts_all), 1)
    onehot = (flat_routes[:, None] == expert_ids).astype(jnp.int32)
    slots = jnp.sum((jnp.cumsum(onehot, axis=0) - onehot) * onehot, axis=1)
    expert_grid = lax.broadcasted_iota(jnp.int32, (experts_all, capacity, 1), 0)
    slot_grid = lax.broadcasted_iota(jnp.int32, (experts_all, capacity, 1), 1)
    match = (
        (flat_routes[None, None, :] == expert_grid) & (slots[None, None, :] == slot_grid)
    ).astype(jnp.bfloat16)
    source_rows = jnp.repeat(normed_moe, TOPK, axis=0)
    outgoing = jnp.einsum(
        "ecr,rd->ecd", match, source_rows, preferred_element_type=jnp.float32
    ).astype(jnp.bfloat16)
    arrived = lax.all_to_all(outgoing, "ep", split_axis=0, concat_axis=0, tiled=True)
    slot_count = arrived.shape[1]
    grouped_in = arrived.reshape(n_ep, local_experts, slot_count, arrived.shape[2])
    gate_h = jnp.einsum(
        "secd,edf->secf", grouped_in, gate_experts, preferred_element_type=jnp.float32
    )
    up_h = jnp.einsum("secd,edf->secf", grouped_in, up_experts, preferred_element_type=jnp.float32)
    hidden_e = (jax.nn.silu(gate_h) * up_h).astype(jnp.bfloat16)
    down_h = jnp.einsum(
        "secf,efd->secd", hidden_e, down_experts, preferred_element_type=jnp.float32
    ).astype(jnp.bfloat16)
    summed = (
        lax.psum_scatter(down_h, "tp", scatter_dimension=3, tiled=True)
        .astype(jnp.float32)
        .astype(jnp.bfloat16)
    )
    summed = summed.reshape(n_ep * local_experts, slot_count, summed.shape[3])
    returned = lax.all_to_all(summed, "ep", split_axis=0, concat_axis=0, tiled=True)
    gathered_back = jnp.einsum("ecr,ecd->rd", match, returned, preferred_element_type=jnp.float32)
    col_width = gathered_back.shape[1]
    weighted = gathered_back.reshape(tok_count, TOPK, col_width) * route_weights[:, :, None]
    routed = jnp.sum(weighted, axis=1)
    own_cols = lax.dynamic_slice_in_dim(resid_mid, lax.axis_index("tp") * col_width, col_width, 1)
    layer_out = (own_cols.astype(jnp.float32) + shared_out + routed).astype(jnp.bfloat16)
    return (layer_out, new_rows)


MESH = pl.DeviceIdType.MESH
ROWS = 16
SLOTS = 8
BF = jnp.bfloat16
F32 = jnp.float32


def fdot(a, b):
    return jnp.dot(a, b, preferred_element_type=F32)


def iota(shape, dim):
    return lax.broadcasted_iota(jnp.int32, shape, dim)


def layer_kernel(
    n, n_tp, tok, resid, g_attn, g_moe, offs, lens, routes, rweights,
    wq_h, wk_h, wv_h, kv_h, wo_h, ge_h, ue_h, de_h, gs_h, us_h, ds_h,
    out, new_rows,
    wqkv, kv, wo, ge, ue, de, gus, dsh,
    x32, xs, xr, p2s, p2r, sc, st, oh, ags, agr, p5s, p5r, rm, dsp, dsr, nss, nsr,
    s1s, s1r, hs, hr, fs, fr, f2s, f2r, rts, rws,
    lsem, s_p1, r_p1, s_p2, r_p2, s_ag, r_ag, s_p5, r_p5, s_d, r_d, s_n, r_n,
    s_s1, r_s1, s_s2, r_s2, s_f, r_f, s_f2, r_f2,
):
    me = lax.axis_index("ep")
    tp = lax.axis_index("tp")
    d_model = x32.shape[1]
    width = d_model // n
    qcols = wq_h.shape[1]
    kcols = wk_h.shape[1]
    heads = offs.shape[1]
    kv_local = kcols // HEAD
    per_group = heads // kv_local
    span = kv_h.shape[1]
    allrows = n * ROWS

    loads = []

    def load(src, dst):
        copy = pltpu.make_async_copy(src, dst, lsem.at[len(loads)])
        copy.start()
        loads.append(copy)
        return copy

    l_qkv = [
        load(wq_h, wqkv.at[:, pl.ds(0, qcols)]),
        load(wk_h, wqkv.at[:, pl.ds(qcols, kcols)]),
        load(wv_h, wqkv.at[:, pl.ds(qcols + kcols, kcols)]),
    ]
    l_kv = [load(kv_h.at[s], kv.at[s]) for s in range(tok)]
    l_wo = load(wo_h, wo)
    fs_cols = gs_h.shape[1]
    l_gus = [load(gs_h, gus.at[:, pl.ds(0, fs_cols)]), load(us_h, gus.at[:, pl.ds(fs_cols, fs_cols)])]
    l_exp = [load(ge_h.at[0], ge), load(ue_h.at[0], ue), load(de_h.at[0], de)]
    l_ds = load(ds_h, dsh)

    barrier = pltpu.get_barrier_semaphore()
    for t in range(n_tp):
        for k in range(n):
            if t or k:
                pl.semaphore_signal(
                    barrier,
                    inc=1,
                    device_id={"ep": lax.rem(me + k, n), "tp": lax.rem(tp + t, n_tp)},
                    device_id_type=MESH,
                )

    x32[...] = jnp.zeros_like(x32)
    x32[0:tok, :] = resid[...].astype(F32)
    for j in range(n):
        xs[j] = x32[:, j * width : (j + 1) * width].astype(BF)
    xr[me] = xs[me]
    rts[...] = jnp.full(rts.shape, -1, jnp.int32)
    rts[:, 0:tok] = routes[...]
    rws[...] = jnp.zeros_like(rws)
    rws[:, 0:tok] = rweights[...]

    pl.semaphore_wait(barrier, n * n_tp - 1)

    sent = []

    def exchange(src, dst, ssem, rsem):
        arrivals = []
        for k in range(1, n):
            peer = lax.rem(me + k, n)
            copy = pltpu.make_async_remote_copy(
                src_ref=src(peer), dst_ref=dst(me), send_sem=ssem.at[k], recv_sem=rsem.at[k],
                device_id={"ep": peer}, device_id_type=MESH,
            )
            copy.start()
            sent.append(copy)
            origin = lax.rem(me + n - k, n)
            arrivals.append(
                pltpu.make_async_remote_copy(
                    src_ref=src(peer), dst_ref=dst(origin), send_sem=ssem.at[k], recv_sem=rsem.at[k],
                    device_id={"ep": peer}, device_id_type=MESH,
                )
            )
        return arrivals

    def exchange_tp(src, dst, ssem, rsem):
        arrivals = []
        for k in range(n):
            for t in range(n_tp):
                if not (k or t):
                    continue
                peer = lax.rem(me + k, n)
                peer_tp = lax.rem(tp + t, n_tp)
                origin = lax.rem(me + n - k, n)
                origin_tp = lax.rem(tp + n_tp - t, n_tp)
                i = t * n + k
                device = {"ep": peer, "tp": peer_tp}
                copy = pltpu.make_async_remote_copy(
                    src_ref=src(peer_tp, peer), dst_ref=dst(tp, me), send_sem=ssem.at[i],
                    recv_sem=rsem.at[i], device_id=device, device_id_type=MESH,
                )
                copy.start()
                sent.append(copy)
                arrivals.append(
                    pltpu.make_async_remote_copy(
                        src_ref=src(peer_tp, peer), dst_ref=dst(origin_tp, origin), send_sem=ssem.at[i],
                        recv_sem=rsem.at[i], device_id=device, device_id_type=MESH,
                    )
                )
        return arrivals

    def arrive(arrivals):
        for copy in arrivals:
            copy.wait_recv()

    got = exchange(lambda j: xs.at[j], lambda j: xr.at[j], s_p1, r_p1)
    inv_attn = lax.rsqrt(jnp.sum(x32[...] * x32[...], axis=1, keepdims=True) / d_model + EPS)
    for copy in l_qkv:
        copy.wait()
    arrive(got)
    gain_a = g_attn[:, pl.ds(pl.multiple_of(me * width, 128), width)]
    scaled = (xr[...].reshape(allrows, width).astype(F32) * gain_a).astype(BF)
    p2s[...] = fdot(scaled, wqkv[...]).astype(BF).reshape(p2s.shape)
    p2r[me] = p2s[me]
    got = exchange(lambda j: p2s.at[j], lambda j: p2r.at[j], s_p2, r_p2)

    row = iota((tok * heads, 1), 0)
    head_of_row = lax.rem(row, heads)
    seq_of_row = row // heads
    off_col = jnp.sum(
        jnp.where(iota((tok * heads, heads), 1) == head_of_row, jnp.broadcast_to(offs[...], (tok * heads, heads)), 0.0),
        axis=1, keepdims=True,
    )
    len_col = jnp.sum(
        jnp.where(iota((tok * heads, tok), 1) == seq_of_row, jnp.broadcast_to(lens[...], (tok * heads, tok)).astype(F32), 0.0),
        axis=1, keepdims=True,
    )
    group_col = head_of_row // per_group
    fold = (lax.rem(iota((qcols, 2 * HEAD), 0), HEAD) == iota((qcols, 2 * HEAD), 1)).astype(F32).astype(BF)
    unfold = (lax.rem(iota((2 * HEAD, qcols), 1), HEAD) + HEAD == iota((2 * HEAD, qcols), 0)).astype(F32).astype(BF)
    head_mask = (iota((1, heads, qcols), 2) // HEAD == iota((1, heads, qcols), 1)).astype(F32)
    blk = 2 * 128
    later = (iota((blk, blk), 0) > iota((blk, blk), 1)).astype(F32).astype(BF)
    oh[...] = jnp.zeros_like(oh)

    arrive(got)
    qkv = jnp.sum(p2r[...].astype(F32), axis=0) * inv_attn
    q = qkv[:, :qcols].astype(BF).astype(F32)
    key = qkv[:, qcols : qcols + kcols]
    val = qkv[:, qcols + kcols :]
    parts = []
    for g in range(kv_local):
        parts += [key[:, g * HEAD : (g + 1) * HEAD], val[:, g * HEAD : (g + 1) * HEAD]]
    new_rows[...] = jnp.concatenate(parts, axis=1)[0:tok, :].astype(BF)

    spread = (q[:, None, :] * head_mask).reshape(ROWS * heads, qcols).astype(BF)
    q8 = fdot(spread, fold) * HEAD ** (-0.5)
    for s in range(tok):
        l_kv[s].wait()
        sc[s * heads : (s + 1) * heads, :] = lax.dot_general(
            q8[s * heads : (s + 1) * heads, :].astype(BF), kv[s],
            (((1,), (1,)), ((), ())), preferred_element_type=F32,
        )
    carry = jnp.zeros((tok * heads, 1), F32)
    for b in reversed(range(span // blk)):
        x = sc[:, b * blk : (b + 1) * blk] - off_col
        where_to = iota((tok * heads, blk), 1) + b * blk
        alive = ((where_to // kv_local).astype(F32) < len_col) & (lax.rem(where_to, kv_local) == group_col)
        tail = jnp.log(1.0 + jnp.exp(-jnp.abs(x)))
        remain = jnp.where(alive, -(jnp.maximum(x, 0.0) + tail), 0.0)
        high = remain.astype(BF)
        low = (remain - high.astype(F32)).astype(BF)
        suffix = fdot(high, later) + fdot(low, later) + carry
        st[:, b * blk : (b + 1) * blk] = jnp.where(alive, jnp.exp(jnp.minimum(x, 0.0) - tail + suffix), 0.0)
        carry = carry + jnp.sum(remain, axis=1, keepdims=True)
    for s in range(tok):
        oh[s * heads : (s + 1) * heads, :] = fdot(st[s * heads : (s + 1) * heads, :].astype(BF), kv[s])
    wide = fdot(oh[...].astype(BF), unfold).reshape(ROWS, heads, qcols) * head_mask
    ags[...] = jnp.sum(wide, axis=1).astype(BF)
    agr[me] = ags[...]
    got = exchange(lambda j: ags, lambda j: agr.at[j], s_ag, r_ag)
    l_wo.wait()

    cgrid = iota((n * SLOTS, ROWS), 0)
    named = jnp.zeros((n * SLOTS, ROWS), F32)
    weight = jnp.zeros((n * SLOTS, ROWS), F32)
    for k in range(TOPK):
        hit = rts[k : k + 1, :] == cgrid // SLOTS
        named = named + jnp.where(hit, 1.0, 0.0)
        weight = weight + jnp.where(hit, jnp.broadcast_to(rws[k : k + 1, :], hit.shape), 0.0)
    before = (iota((ROWS, ROWS), 0) < iota((ROWS, ROWS), 1)).astype(F32).astype(BF)
    slot = fdot(named.astype(BF), before)
    pick = jnp.where(slot == lax.rem(cgrid, SLOTS).astype(F32), named, 0.0)
    weight = weight * pick
    pick = pick.astype(BF)

    arrive(got)
    p5s[...] = fdot(agr[...].reshape(allrows, qcols), wo[...]).astype(BF).reshape(p5s.shape)
    p5r[tp, me] = p5s[me]
    arrive(exchange_tp(lambda t, j: p5s.at[j], lambda t, j: p5r.at[t, j], s_p5, r_p5))

    square = jnp.zeros((ROWS, 1), F32)
    for j in range(n):
        added = x32[:, j * width : (j + 1) * width]
        attn = p5r[0, j].astype(F32)
        for t in range(1, n_tp):
            attn = attn + p5r[t, j].astype(F32)
        mid = (added + attn).astype(BF).astype(F32)
        rm[j] = mid
        square = square + jnp.sum(mid * mid, axis=1, keepdims=True)
    inv_moe = lax.rsqrt(square / d_model + EPS)
    for j in range(n):
        nss[j] = (rm[j] * inv_moe * g_moe[:, j * width : (j + 1) * width]).astype(BF)
    nsr[me] = nss[me]
    got_n = exchange(lambda j: nss.at[j], lambda j: nsr.at[j], s_n, r_n)
    for j in range(n):
        dsp[:, :, j * width : (j + 1) * width] = fdot(pick, nss[j]).reshape(n, SLOTS, width).astype(BF)
    dsr[me] = dsp[me]
    got_d = exchange(lambda j: dsp.at[j], lambda j: dsr.at[j], s_d, r_d)

    for copy in l_gus:
        copy.wait()
    arrive(got_n)
    s1s[...] = fdot(nsr[...].reshape(allrows, width), gus[...]).astype(BF).reshape(s1s.shape)
    s1r[me] = s1s[me]
    got_s1 = exchange(lambda j: s1s.at[j], lambda j: s1r.at[j], s_s1, r_s1)
    for copy in l_exp:
        copy.wait()
    l_ds.wait()
    arrive(got_s1)
    both = jnp.sum(s1r[...].astype(F32), axis=0)
    hs[...] = (jax.nn.silu(both[:, :fs_cols]) * both[:, fs_cols:]).astype(BF)
    hr[me] = hs[...]
    got_s2 = exchange(lambda j: hs, lambda j: hr.at[j], s_s2, r_s2)

    arrive(got_d)
    rows_in = dsr[...].astype(F32).reshape(n * SLOTS, d_model).astype(BF)
    hidden = (jax.nn.silu(fdot(rows_in, ge[...])) * fdot(rows_in, ue[...])).astype(BF)
    half = d_model // n_tp
    for t in range(n_tp):
        fs[t] = fdot(hidden, de[:, t * half : (t + 1) * half]).reshape(n, SLOTS, half).astype(BF)
    fr[tp, me] = fs[tp, me]
    got_f = exchange_tp(lambda t, j: fs.at[t, j], lambda t, j: fr.at[t, j], s_f, r_f)

    arrive(got_s2)
    f2s[...] = fdot(hr[...].reshape(allrows, fs_cols), dsh[...]).astype(BF).reshape(f2s.shape)
    f2r[tp, me] = f2s[me]
    got_f2 = exchange_tp(lambda t, j: f2s.at[j], lambda t, j: f2r.at[t, j], s_f2, r_f2)
    arrive(got_f)
    back = fr[0].astype(F32)
    for t in range(1, n_tp):
        back = back + fr[t].astype(F32)
    back = back.astype(BF).astype(F32).reshape(n * SLOTS, half)
    routed = lax.dot_general(
        weight, back, (((0,), (0,)), ((), ())), preferred_element_type=F32, precision=lax.Precision.HIGHEST
    )
    arrive(got_f2)
    chunks = n // n_tp
    for c in range(chunks):
        j = tp * chunks + c
        shared = f2r[0, j].astype(F32)
        for t in range(1, n_tp):
            shared = shared + f2r[t, j].astype(F32)
        total = rm[j] + shared + routed[:, c * width : (c + 1) * width]
        out[:, c * width : (c + 1) * width] = total[0:tok, :].astype(BF)
    for copy in sent:
        copy.wait_send()


def fused(
    resid_in, norm_attn, norm_moe, w_query, w_key, w_value, head_offset, kv_cache, lengths,
    w_output, routes, route_weights, gate_experts, up_experts, down_experts,
    gate_shared, up_shared, down_shared,
):
    n = lax.axis_size("ep")
    n_tp = lax.axis_size("tp")
    tok, d_model = resid_in.shape
    width = d_model // n
    qcols, kcols = w_query.shape[1], w_key.shape[1]
    heads = head_offset.shape[0]
    length, kv_local = kv_cache.shape[1:3]
    span = length * kv_local
    fe, fs_cols = gate_experts.shape[2], gate_shared.shape[1]
    half = d_model // n_tp
    qkv = qcols + 2 * kcols
    V = pltpu.VMEM
    dma = pltpu.SemaphoreType.DMA
    scratch = [
        V((width, qkv), BF), V((tok, span, 2 * HEAD), BF), V(w_output.shape, BF),
        V((d_model, fe), BF), V((d_model, fe), BF), V((fe, d_model), BF),
        V((width, 2 * fs_cols), BF), V(down_shared.shape, BF),
        V((ROWS, d_model), F32), V((n, ROWS, width), BF), V((n, ROWS, width), BF),
        V((n, ROWS, qkv), BF), V((n, ROWS, qkv), BF),
        V((tok * heads, span), F32), V((tok * heads, span), F32), V((ROWS * heads, 2 * HEAD), F32),
        V((ROWS, qcols), BF), V((n, ROWS, qcols), BF),
        V((n, ROWS, width), BF), V((n_tp, n, ROWS, width), BF), V((n, ROWS, width), F32),
        V((n, SLOTS, d_model), BF), V((n, SLOTS, d_model), BF),
        V((n, ROWS, width), BF), V((n, ROWS, width), BF),
        V((n, ROWS, 2 * fs_cols), BF), V((n, ROWS, 2 * fs_cols), BF),
        V((ROWS, fs_cols), BF), V((n, ROWS, fs_cols), BF),
        V((n_tp, n, SLOTS, half), BF), V((n_tp, n, SLOTS, half), BF),
        V((n, ROWS, width), BF), V((n_tp, n, ROWS, width), BF),
        V((TOPK, ROWS), jnp.int32), V((TOPK, ROWS), F32),
        dma((10 + tok,)),
    ]
    scratch += [dma((n,))] * 6 + [dma((n_tp * n,))] * 2 + [dma((n,))] * 8 + [dma((n_tp * n,))] * 4
    in_vmem = pl.BlockSpec(memory_space=pltpu.VMEM)
    in_hbm = pl.BlockSpec(memory_space=pl.ANY)
    out, rows = pl.pallas_call(
        functools.partial(layer_kernel, n, n_tp, tok),
        out_shape=(
            jax.ShapeDtypeStruct((tok, half), BF),
            jax.ShapeDtypeStruct((tok, 2 * kcols), BF),
        ),
        in_specs=[in_vmem] * 7 + [in_hbm] * 11,
        out_specs=(in_vmem, in_vmem),
        scratch_shapes=scratch,
        compiler_params=pltpu.CompilerParams(
            collective_id=0, has_side_effects=True, vmem_limit_bytes=60 * 2**20
        ),
    )(
        resid_in, norm_attn.reshape(1, -1), norm_moe.reshape(1, -1), head_offset.reshape(1, -1),
        lengths.reshape(1, -1), routes.T, route_weights.T,
        w_query, w_key, w_value, kv_cache.reshape(tok, span, 2 * HEAD), w_output,
        gate_experts, up_experts, down_experts, gate_shared, up_shared, down_shared,
    )
    return out, rows.reshape(tok, kv_local, 2 * HEAD)


def layer(*args):
    n = lax.axis_size("ep")
    n_tp = lax.axis_size("tp")
    tok, d_model = args[0].shape
    local_experts = args[12].shape[0]
    capacity = min(tok, tok * TOPK // (local_experts * n) + 2)
    fits = (
        tok <= ROWS
        and local_experts == 1
        and capacity <= SLOTS
        and d_model % (128 * n) == 0
        and n % n_tp == 0
    )
    return fused(*args) if fits else on_device(*args)


def solution(mesh):
    return jax.shard_map(
        layer,
        mesh=mesh,
        in_specs=(
            P(("grp", "ep"), None),
            P(),
            P(),
            P("ep", "tp"),
            P("ep", "tp"),
            P("ep", "tp"),
            P("tp"),
            P(("grp", "ep"), None, "tp", None),
            P(("grp", "ep")),
            P("tp", "ep"),
            P(("grp", "ep"), None),
            P(("grp", "ep"), None),
            P("ep", None, "tp"),
            P("ep", None, "tp"),
            P("ep", "tp", None),
            P("ep", "tp"),
            P("ep", "tp"),
            P("tp", "ep"),
        ),
        out_specs=(P(("grp", "ep"), "tp"), P(("grp", "ep"), "tp", None)),
        check_vma=False,
    )
```

```python
import functools

import jax
import jax.numpy as jnp
from jax import lax
from jax.experimental import pallas as pl
from jax.experimental.pallas import tpu as pltpu
from jax.sharding import PartitionSpec as P

HEAD = 64
TOPK = 4


EPS = 1e-06


def rms_scale(row_block, gain):
    rows_wide = row_block.astype(jnp.float32)
    inverse = lax.rsqrt(jnp.mean(rows_wide * rows_wide, axis=-1, keepdims=True) + EPS)
    return rows_wide * inverse * gain


def stick_read(query, kv_cache, lengths, offsets):
    seq_count = query.shape[0]
    kv_local = kv_cache.shape[2]
    head_local = offsets.shape[0]
    per_group = head_local // kv_local
    cache_len = kv_cache.shape[1]
    grouped = query.reshape(seq_count, kv_local, per_group, HEAD)
    key_rows = kv_cache[:, :, :, :HEAD]
    value_rows = kv_cache[:, :, :, HEAD:]
    scores = jnp.einsum("skgd,slkd->skgl", grouped, key_rows, preferred_element_type=jnp.float32)
    scores = scores * HEAD ** (-0.5) - offsets.reshape(1, kv_local, per_group, 1)
    positions = lax.broadcasted_iota(jnp.int32, (seq_count, cache_len), 1)
    alive_mask = (positions < lengths[:, None])[:, None, None, :]
    remain = jnp.where(alive_mask, jax.nn.log_sigmoid(-scores), 0.0)
    suffix = lax.cumsum(remain, axis=3, reverse=True) - remain
    stick = jnp.where(alive_mask, jnp.exp(jax.nn.log_sigmoid(scores) + suffix), 0.0).astype(
        jnp.bfloat16
    )
    mixed_out = jnp.einsum("skgl,slkd->skgd", stick, value_rows, preferred_element_type=jnp.float32)
    return mixed_out.reshape(seq_count, head_local * HEAD).astype(jnp.bfloat16)


def on_device(
    resid_in,
    norm_attn,
    norm_moe,
    w_query,
    w_key,
    w_value,
    head_offset,
    kv_cache,
    lengths,
    w_output,
    routes,
    route_weights,
    gate_experts,
    up_experts,
    down_experts,
    gate_shared,
    up_shared,
    down_shared,
):
    tok_count = resid_in.shape[0]
    n_ep = lax.axis_size("ep")
    normed = rms_scale(resid_in, norm_attn).astype(jnp.bfloat16)
    k_cols = w_key.shape[1]
    pieces = (
        lax.all_gather(w_query, "ep", axis=0, tiled=True),
        lax.all_gather(w_key, "ep", axis=0, tiled=True),
        lax.all_gather(w_value, "ep", axis=0, tiled=True),
    )
    sliced = normed
    query_f, key_f, value_f = tuple(
        (
            jnp.dot(sliced, weight_piece, preferred_element_type=jnp.float32)
            for weight_piece in pieces
        )
    )
    query = query_f.astype(jnp.bfloat16)
    kv_local = k_cols // HEAD
    key_new = key_f.astype(jnp.bfloat16).reshape(tok_count, kv_local, HEAD)
    value_new = value_f.astype(jnp.bfloat16).reshape(tok_count, kv_local, HEAD)
    new_rows = jnp.concatenate([key_new, value_new], axis=2)
    attended = stick_read(query, kv_cache, lengths, head_offset)
    attn_part = jnp.dot(
        attended,
        lax.all_gather(w_output, "ep", axis=1, tiled=True),
        preferred_element_type=jnp.float32,
    ).astype(jnp.bfloat16)
    attn_sum = lax.psum(attn_part, "tp").astype(jnp.float32)
    resid_mid = (resid_in.astype(jnp.float32) + attn_sum).astype(jnp.bfloat16)
    normed_moe = rms_scale(resid_mid, norm_moe).astype(jnp.bfloat16)
    pieces = (
        lax.all_gather(gate_shared, "ep", axis=0, tiled=True),
        lax.all_gather(up_shared, "ep", axis=0, tiled=True),
    )
    sliced = normed_moe
    gate_s = jnp.dot(sliced, pieces[0], preferred_element_type=jnp.float32)
    up_s = jnp.dot(sliced, pieces[1], preferred_element_type=jnp.float32)
    hidden_shared = (jax.nn.silu(gate_s) * up_s).astype(jnp.bfloat16)
    shared_part = jnp.dot(
        hidden_shared,
        lax.all_gather(down_shared, "ep", axis=1, tiled=True),
        preferred_element_type=jnp.float32,
    ).astype(jnp.bfloat16)
    shared_out = lax.psum_scatter(shared_part, "tp", scatter_dimension=1, tiled=True).astype(
        jnp.float32
    )
    local_experts = gate_experts.shape[0]
    experts_all = local_experts * n_ep
    capacity = min(tok_count, tok_count * TOPK // experts_all + 2)
    flat_routes = routes.reshape(-1)
    expert_ids = lax.broadcasted_iota(jnp.int32, (1, experts_all), 1)
    onehot = (flat_routes[:, None] == expert_ids).astype(jnp.int32)
    slots = jnp.sum((jnp.cumsum(onehot, axis=0) - onehot) * onehot, axis=1)
    expert_grid = lax.broadcasted_iota(jnp.int32, (experts_all, capacity, 1), 0)
    slot_grid = lax.broadcasted_iota(jnp.int32, (experts_all, capacity, 1), 1)
    match = (
        (flat_routes[None, None, :] == expert_grid) & (slots[None, None, :] == slot_grid)
    ).astype(jnp.bfloat16)
    source_rows = jnp.repeat(normed_moe, TOPK, axis=0)
    outgoing = jnp.einsum(
        "ecr,rd->ecd", match, source_rows, preferred_element_type=jnp.float32
    ).astype(jnp.bfloat16)
    arrived = lax.all_to_all(outgoing, "ep", split_axis=0, concat_axis=0, tiled=True)
    slot_count = arrived.shape[1]
    grouped_in = arrived.reshape(n_ep, local_experts, slot_count, arrived.shape[2])
    gate_h = jnp.einsum(
        "secd,edf->secf", grouped_in, gate_experts, preferred_element_type=jnp.float32
    )
    up_h = jnp.einsum("secd,edf->secf", grouped_in, up_experts, preferred_element_type=jnp.float32)
    hidden_e = (jax.nn.silu(gate_h) * up_h).astype(jnp.bfloat16)
    down_h = jnp.einsum(
        "secf,efd->secd", hidden_e, down_experts, preferred_element_type=jnp.float32
    ).astype(jnp.bfloat16)
    summed = (
        lax.psum_scatter(down_h, "tp", scatter_dimension=3, tiled=True)
        .astype(jnp.float32)
        .astype(jnp.bfloat16)
    )
    summed = summed.reshape(n_ep * local_experts, slot_count, summed.shape[3])
    returned = lax.all_to_all(summed, "ep", split_axis=0, concat_axis=0, tiled=True)
    gathered_back = jnp.einsum("ecr,ecd->rd", match, returned, preferred_element_type=jnp.float32)
    col_width = gathered_back.shape[1]
    weighted = gathered_back.reshape(tok_count, TOPK, col_width) * route_weights[:, :, None]
    routed = jnp.sum(weighted, axis=1)
    own_cols = lax.dynamic_slice_in_dim(resid_mid, lax.axis_index("tp") * col_width, col_width, 1)
    layer_out = (own_cols.astype(jnp.float32) + shared_out + routed).astype(jnp.bfloat16)
    return (layer_out, new_rows)


MESH = pl.DeviceIdType.MESH
ROWS = 16
SLOTS = 8
BF = jnp.bfloat16
F32 = jnp.float32


def fdot(a, b):
    return jnp.dot(a, b, preferred_element_type=F32)


def iota(shape, dim):
    return lax.broadcasted_iota(jnp.int32, shape, dim)


def layer_kernel(
    n, n_tp, tok, resid, g_attn, g_moe, offs, lens, routes, rweights,
    wq_h, wk_h, wv_h, kv_h, wo_h, ge_h, ue_h, de_h, gs_h, us_h, ds_h,
    out, new_rows,
    wqkv, kv, wo, ge, ue, de, gus, dsh,
    x32, xs, xr, p2s, p2r, sc, st, oh, ags, agr, xps, xpr, dsp, dsr,
    s1s, s1r, hs, hr, fs, fr, f2s, f2r, rts, rws,
    lsem, s_p1, r_p1, s_p2, r_p2, s_ag, r_ag, s_x, r_x, s_d, r_d,
    s_s1, r_s1, s_s2, r_s2, s_f, r_f, s_f2, r_f2,
):
    me = lax.axis_index("ep")
    tp = lax.axis_index("tp")
    d_model = x32.shape[1]
    width = d_model // n
    qcols = wq_h.shape[1]
    kcols = wk_h.shape[1]
    heads = offs.shape[1]
    kv_local = kcols // HEAD
    per_group = heads // kv_local
    span = kv_h.shape[1]
    allrows = n * ROWS

    loads = []

    def load(src, dst):
        copy = pltpu.make_async_copy(src, dst, lsem.at[len(loads)])
        copy.start()
        loads.append(copy)
        return copy

    l_qkv = [
        load(wq_h, wqkv.at[:, pl.ds(0, qcols)]),
        load(wk_h, wqkv.at[:, pl.ds(qcols, kcols)]),
        load(wv_h, wqkv.at[:, pl.ds(qcols + kcols, kcols)]),
    ]
    l_kv = [load(kv_h.at[s], kv.at[s]) for s in range(tok)]
    l_wo = load(wo_h, wo)
    fs_cols = gs_h.shape[1]
    l_gus = [load(gs_h, gus.at[:, pl.ds(0, fs_cols)]), load(us_h, gus.at[:, pl.ds(fs_cols, fs_cols)])]
    l_exp = [load(ge_h.at[0], ge), load(ue_h.at[0], ue), load(de_h.at[0], de)]
    l_ds = load(ds_h, dsh)

    barrier = pltpu.get_barrier_semaphore()
    for t in range(n_tp):
        for k in range(n):
            if t or k:
                pl.semaphore_signal(
                    barrier,
                    inc=1,
                    device_id={"ep": lax.rem(me + k, n), "tp": lax.rem(tp + t, n_tp)},
                    device_id_type=MESH,
                )

    x32[...] = jnp.zeros_like(x32)
    x32[0:tok, :] = resid[...].astype(F32)
    rts[...] = jnp.full(rts.shape, -1.0, F32)
    rts[:, 0:tok] = routes[...].astype(F32)
    rws[...] = jnp.zeros_like(rws)
    rws[:, 0:tok] = rweights[...]
    spot = (iota((TOPK, 128), 0) == iota((TOPK, 128), 1)).astype(F32)
    routes_rows = lax.dot_general(
        rts[...], spot, (((0,), (0,)), ((), ())), preferred_element_type=F32
    ).astype(BF)
    for j in range(n):
        xs[j, :, 0:width] = x32[:, j * width : (j + 1) * width].astype(BF)
        xs[j, :, width:] = routes_rows
    xr[me] = xs[me]

    pl.semaphore_wait(barrier, n * n_tp - 1)

    sent = []

    def exchange(src, dst, ssem, rsem):
        arrivals = []
        for k in range(1, n):
            peer = lax.rem(me + k, n)
            copy = pltpu.make_async_remote_copy(
                src_ref=src(peer), dst_ref=dst(me), send_sem=ssem.at[k], recv_sem=rsem.at[k],
                device_id={"ep": peer}, device_id_type=MESH,
            )
            copy.start()
            sent.append(copy)
            origin = lax.rem(me + n - k, n)
            arrivals.append(
                pltpu.make_async_remote_copy(
                    src_ref=src(peer), dst_ref=dst(origin), send_sem=ssem.at[k], recv_sem=rsem.at[k],
                    device_id={"ep": peer}, device_id_type=MESH,
                )
            )
        return arrivals

    def exchange_tp(src, dst, ssem, rsem):
        arrivals = []
        for k in range(n):
            for t in range(n_tp):
                if not (k or t):
                    continue
                peer = lax.rem(me + k, n)
                peer_tp = lax.rem(tp + t, n_tp)
                origin = lax.rem(me + n - k, n)
                origin_tp = lax.rem(tp + n_tp - t, n_tp)
                i = t * n + k
                device = {"ep": peer, "tp": peer_tp}
                copy = pltpu.make_async_remote_copy(
                    src_ref=src(peer_tp, peer), dst_ref=dst(tp, me), send_sem=ssem.at[i],
                    recv_sem=rsem.at[i], device_id=device, device_id_type=MESH,
                )
                copy.start()
                sent.append(copy)
                arrivals.append(
                    pltpu.make_async_remote_copy(
                        src_ref=src(peer_tp, peer), dst_ref=dst(origin_tp, origin), send_sem=ssem.at[i],
                        recv_sem=rsem.at[i], device_id=device, device_id_type=MESH,
                    )
                )
        return arrivals

    def arrive(arrivals):
        for copy in arrivals:
            copy.wait_recv()

    got = exchange(lambda j: xs.at[j], lambda j: xr.at[j], s_p1, r_p1)
    inv_attn = lax.rsqrt(jnp.sum(x32[...] * x32[...], axis=1, keepdims=True) / d_model + EPS)
    for copy in l_qkv:
        copy.wait()
    arrive(got)
    gain_a = g_attn[:, pl.ds(pl.multiple_of(me * width, 128), width)]
    scaled = (xr[:, :, 0:width].reshape(allrows, width).astype(F32) * gain_a).astype(BF)
    p2s[...] = fdot(scaled, wqkv[...]).astype(BF).reshape(p2s.shape)
    p2r[me] = p2s[me]
    got = exchange(lambda j: p2s.at[j], lambda j: p2r.at[j], s_p2, r_p2)

    row = iota((tok * heads, 1), 0)
    head_of_row = lax.rem(row, heads)
    seq_of_row = row // heads
    off_col = jnp.sum(
        jnp.where(iota((tok * heads, heads), 1) == head_of_row, jnp.broadcast_to(offs[...], (tok * heads, heads)), 0.0),
        axis=1, keepdims=True,
    )
    len_col = jnp.sum(
        jnp.where(iota((tok * heads, tok), 1) == seq_of_row, jnp.broadcast_to(lens[...], (tok * heads, tok)).astype(F32), 0.0),
        axis=1, keepdims=True,
    )
    group_col = head_of_row // per_group
    fold = (lax.rem(iota((qcols, 2 * HEAD), 0), HEAD) == iota((qcols, 2 * HEAD), 1)).astype(F32).astype(BF)
    unfold = (lax.rem(iota((2 * HEAD, qcols), 1), HEAD) + HEAD == iota((2 * HEAD, qcols), 0)).astype(F32).astype(BF)
    head_mask = (iota((1, heads, qcols), 2) // HEAD == iota((1, heads, qcols), 1)).astype(F32)
    blk = 2 * 128
    later = (iota((blk, blk), 0) > iota((blk, blk), 1)).astype(F32).astype(BF)
    oh[...] = jnp.zeros_like(oh)

    arrive(got)
    qkv = jnp.sum(p2r[...].astype(F32), axis=0) * inv_attn
    q = qkv[:, :qcols].astype(BF).astype(F32)
    key = qkv[:, qcols : qcols + kcols]
    val = qkv[:, qcols + kcols :]
    parts = []
    for g in range(kv_local):
        parts += [key[:, g * HEAD : (g + 1) * HEAD], val[:, g * HEAD : (g + 1) * HEAD]]
    new_rows[...] = jnp.concatenate(parts, axis=1)[0:tok, :].astype(BF)

    spread = (q[:, None, :] * head_mask).reshape(ROWS * heads, qcols).astype(BF)
    q8 = fdot(spread, fold) * HEAD ** (-0.5)
    for s in range(tok):
        l_kv[s].wait()
        sc[s * heads : (s + 1) * heads, :] = lax.dot_general(
            q8[s * heads : (s + 1) * heads, :].astype(BF), kv[s],
            (((1,), (1,)), ((), ())), preferred_element_type=F32,
        )
    carry = jnp.zeros((tok * heads, 1), F32)
    for b in reversed(range(span // blk)):
        x = sc[:, b * blk : (b + 1) * blk] - off_col
        where_to = iota((tok * heads, blk), 1) + b * blk
        alive = ((where_to // kv_local).astype(F32) < len_col) & (lax.rem(where_to, kv_local) == group_col)
        tail = jnp.log(1.0 + jnp.exp(-jnp.abs(x)))
        remain = jnp.where(alive, -(jnp.maximum(x, 0.0) + tail), 0.0)
        high = remain.astype(BF)
        low = (remain - high.astype(F32)).astype(BF)
        suffix = fdot(high, later) + fdot(low, later) + carry
        st[:, b * blk : (b + 1) * blk] = jnp.where(alive, jnp.exp(jnp.minimum(x, 0.0) - tail + suffix), 0.0)
        carry = carry + jnp.sum(remain, axis=1, keepdims=True)
    for s in range(tok):
        oh[s * heads : (s + 1) * heads, :] = fdot(st[s * heads : (s + 1) * heads, :].astype(BF), kv[s])
    wide = fdot(oh[...].astype(BF), unfold).reshape(ROWS, heads, qcols) * head_mask
    ags[...] = jnp.sum(wide, axis=1).astype(BF)
    agr[me] = ags[...]
    got = exchange(lambda j: ags, lambda j: agr.at[j], s_ag, r_ag)
    l_wo.wait()

    cgrid = iota((n * SLOTS, ROWS), 0)
    named = jnp.zeros((n * SLOTS, ROWS), F32)
    weight = jnp.zeros((n * SLOTS, ROWS), F32)
    for k in range(TOPK):
        hit = rts[k : k + 1, :] == (cgrid // SLOTS).astype(F32)
        named = named + jnp.where(hit, 1.0, 0.0)
        weight = weight + jnp.where(hit, jnp.broadcast_to(rws[k : k + 1, :], hit.shape), 0.0)
    before = (iota((ROWS, ROWS), 0) < iota((ROWS, ROWS), 1)).astype(F32).astype(BF)
    slot = fdot(named.astype(BF), before)
    pick = jnp.where(slot == lax.rem(cgrid, SLOTS).astype(F32), named, 0.0)
    weight = weight * pick
    per_expert = n * SLOTS
    all_routes = xr[:, :, width:].reshape(allrows, 128).astype(F32).T
    rgrid = iota((n * per_expert, allrows), 0)
    qgrid = iota((n * per_expert, allrows), 1)
    want = (rgrid // per_expert).astype(F32)
    named_all = jnp.zeros((n * per_expert, allrows), F32)
    for k in range(TOPK):
        named_all = named_all + jnp.where(all_routes[k : k + 1, :] == want, 1.0, 0.0)
    qa, qb = iota((allrows, allrows), 0), iota((allrows, allrows), 1)
    before_all = jnp.where((qa // ROWS == qb // ROWS) & (qa < qb), 1.0, 0.0).astype(BF)
    slot_all = fdot(named_all.astype(BF), before_all)
    right = (lax.rem(rgrid, per_expert) // SLOTS == qgrid // ROWS) & (
        slot_all == lax.rem(rgrid, SLOTS).astype(F32)
    )
    pick_all = jnp.where(right, named_all, 0.0).astype(BF)

    arrive(got)
    part = fdot(agr[...].reshape(allrows, qcols), wo[...]).astype(BF)
    xps[...] = part
    swap = pltpu.make_async_remote_copy(
        src_ref=xps, dst_ref=xpr, send_sem=s_x.at[0], recv_sem=r_x.at[0],
        device_id={"tp": lax.rem(tp + 1, n_tp)}, device_id_type=MESH,
    )
    swap.start()
    sent.append(swap)
    gain_m = g_moe[:, pl.ds(pl.multiple_of(me * width, 128), width)]
    base = xr[:, :, 0:width].reshape(allrows, width).astype(F32)
    for copy in l_gus:
        copy.wait()
    swap.wait_recv()
    mid = (base + (part.astype(F32) + xpr[...].astype(F32))).astype(BF)
    mid32 = mid.astype(F32)

    square = jnp.sum(mid32 * mid32, axis=1, keepdims=True)
    sq_high = square.astype(BF).astype(F32)
    lane = iota((allrows, 128), 1)
    sq_wide = jnp.where(lane == 0, sq_high, jnp.where(lane == 1, square - sq_high, 0.0))
    s1s[:, :, 0 : 2 * fs_cols] = fdot((mid32 * gain_m).astype(BF), gus[...]).astype(BF).reshape(n, ROWS, 2 * fs_cols)
    s1s[:, :, 2 * fs_cols :] = sq_wide.astype(BF).reshape(n, ROWS, 128)
    s1r[me] = s1s[me]
    got_s1 = exchange(lambda j: s1s.at[j], lambda j: s1r.at[j], s_s1, r_s1)
    dsp[...] = fdot(pick_all, mid).astype(BF).reshape(dsp.shape)
    dsr[me] = dsp[me]
    got_d = exchange(lambda j: dsp.at[j], lambda j: dsr.at[j], s_d, r_d)

    for copy in l_exp:
        copy.wait()
    l_ds.wait()
    arrive(got_s1)
    inv_own = lax.rsqrt(
        jnp.sum(jnp.sum(s1r[:, :, 2 * fs_cols :].astype(F32), axis=0), axis=1, keepdims=True) / d_model + EPS
    )
    both = jnp.sum(s1r[:, :, 0 : 2 * fs_cols].astype(F32), axis=0) * inv_own
    hs[...] = (jax.nn.silu(both[:, :fs_cols]) * both[:, fs_cols:]).astype(BF)
    hr[me] = hs[...]
    got_s2 = exchange(lambda j: hs, lambda j: hr.at[j], s_s2, r_s2)

    arrive(got_d)
    square = jnp.zeros((per_expert, 1), F32)
    for j in range(n):
        piece = dsr[j].astype(F32)
        square = square + jnp.sum(piece * piece, axis=1, keepdims=True)
    inv_moe = lax.rsqrt(square / d_model + EPS)
    rows_in = jnp.concatenate(
        [
            (dsr[j].astype(F32) * inv_moe * g_moe[:, j * width : (j + 1) * width]).astype(BF)
            for j in range(n)
        ],
        axis=1,
    )
    hidden = (jax.nn.silu(fdot(rows_in, ge[...])) * fdot(rows_in, ue[...])).astype(BF)
    half = d_model // n_tp
    for t in range(n_tp):
        fs[t] = fdot(hidden, de[:, t * half : (t + 1) * half]).reshape(n, SLOTS, half).astype(BF)
    fr[tp, me] = fs[tp, me]
    got_f = exchange_tp(lambda t, j: fs.at[t, j], lambda t, j: fr.at[t, j], s_f, r_f)

    arrive(got_s2)
    chunks = n // n_tp
    target = me // chunks
    chunk = lax.rem(me, chunks)
    carried = jnp.where(tp == 0, 1.0, 0.0) * mid32
    f2s[...] = (fdot(hr[...].reshape(allrows, fs_cols), dsh[...]) + carried).astype(BF).reshape(f2s.shape)

    def give(k):
        peer = lax.rem(me + k, n)
        return pltpu.make_async_remote_copy(
            src_ref=f2s.at[peer], dst_ref=f2r.at[tp, chunk], send_sem=s_f2.at[k],
            recv_sem=r_f2.at[chunk * n_tp + tp], device_id={"ep": peer, "tp": target}, device_id_type=MESH,
        )

    for k in range(1, n):
        give(k).start()

    @pl.when(target != tp)
    def _():
        give(0).start()

    @pl.when(target == tp)
    def _():
        f2r[tp, chunk] = f2s[me]

    arrive(got_f)
    back = fr[0].astype(F32)
    for t in range(1, n_tp):
        back = back + fr[t].astype(F32)
    back = back.astype(BF).astype(F32).reshape(n * SLOTS, half)
    routed = lax.dot_general(
        weight, back, (((0,), (0,)), ((), ())), preferred_element_type=F32, precision=lax.Precision.HIGHEST
    )
    for c in range(chunks):
        for t in range(n_tp):

            @pl.when((tp * chunks + c != me) | (tp != t))
            def _():
                pltpu.make_async_remote_copy(
                    src_ref=f2s.at[me], dst_ref=f2r.at[t, c], send_sem=s_f2.at[0],
                    recv_sem=r_f2.at[c * n_tp + t], device_id={"tp": 1 - tp}, device_id_type=MESH,
                ).wait_recv()

    for c in range(chunks):
        total = routed[:, c * width : (c + 1) * width]
        for t in range(n_tp):
            total = total + f2r[t, c].astype(F32)
        out[:, c * width : (c + 1) * width] = total[0:tok, :].astype(BF)
    for k in range(1, n):
        give(k).wait_send()

    @pl.when(target != tp)
    def _():
        give(0).wait_send()

    for copy in sent:
        copy.wait_send()


def fused(
    resid_in, norm_attn, norm_moe, w_query, w_key, w_value, head_offset, kv_cache, lengths,
    w_output, routes, route_weights, gate_experts, up_experts, down_experts,
    gate_shared, up_shared, down_shared,
):
    n = lax.axis_size("ep")
    n_tp = lax.axis_size("tp")
    tok, d_model = resid_in.shape
    width = d_model // n
    qcols, kcols = w_query.shape[1], w_key.shape[1]
    heads = head_offset.shape[0]
    length, kv_local = kv_cache.shape[1:3]
    span = length * kv_local
    fe, fs_cols = gate_experts.shape[2], gate_shared.shape[1]
    half = d_model // n_tp
    qkv = qcols + 2 * kcols
    V = pltpu.VMEM
    dma = pltpu.SemaphoreType.DMA
    scratch = [
        V((width, qkv), BF), V((tok, span, 2 * HEAD), BF), V(w_output.shape, BF),
        V((d_model, fe), BF), V((d_model, fe), BF), V((fe, d_model), BF),
        V((width, 2 * fs_cols), BF), V(down_shared.shape, BF),
        V((ROWS, d_model), F32), V((n, ROWS, width + 128), BF), V((n, ROWS, width + 128), BF),
        V((n, ROWS, qkv), BF), V((n, ROWS, qkv), BF),
        V((tok * heads, span), F32), V((tok * heads, span), F32), V((ROWS * heads, 2 * HEAD), F32),
        V((ROWS, qcols), BF), V((n, ROWS, qcols), BF),
        V((n * ROWS, width), BF), V((n * ROWS, width), BF),
        V((n, n * SLOTS, width), BF), V((n, n * SLOTS, width), BF),
        V((n, ROWS, 2 * fs_cols + 128), BF), V((n, ROWS, 2 * fs_cols + 128), BF),
        V((ROWS, fs_cols), BF), V((n, ROWS, fs_cols), BF),
        V((n_tp, n, SLOTS, half), BF), V((n_tp, n, SLOTS, half), BF),
        V((n, ROWS, width), BF), V((n_tp, n // n_tp, ROWS, width), BF),
        V((TOPK, ROWS), F32), V((TOPK, ROWS), F32),
        dma((10 + tok,)),
    ]
    scratch += [dma((n,))] * 6 + [dma((1,))] * 2 + [dma((n,))] * 6 + [dma((n_tp * n,))] * 2 + [dma((n,))] * 2
    in_vmem = pl.BlockSpec(memory_space=pltpu.VMEM)
    in_hbm = pl.BlockSpec(memory_space=pl.ANY)
    out, rows = pl.pallas_call(
        functools.partial(layer_kernel, n, n_tp, tok),
        out_shape=(
            jax.ShapeDtypeStruct((tok, half), BF),
            jax.ShapeDtypeStruct((tok, 2 * kcols), BF),
        ),
        in_specs=[in_vmem] * 7 + [in_hbm] * 11,
        out_specs=(in_vmem, in_vmem),
        scratch_shapes=scratch,
        compiler_params=pltpu.CompilerParams(
            collective_id=0, has_side_effects=True, vmem_limit_bytes=60 * 2**20
        ),
    )(
        resid_in, norm_attn.reshape(1, -1), norm_moe.reshape(1, -1), head_offset.reshape(1, -1),
        lengths.reshape(1, -1), routes.T, route_weights.T,
        w_query, w_key, w_value, kv_cache.reshape(tok, span, 2 * HEAD), w_output,
        gate_experts, up_experts, down_experts, gate_shared, up_shared, down_shared,
    )
    return out, rows.reshape(tok, kv_local, 2 * HEAD)


def layer(*args):
    n = lax.axis_size("ep")
    n_tp = lax.axis_size("tp")
    tok, d_model = args[0].shape
    local_experts = args[12].shape[0]
    experts_all = local_experts * n
    capacity = min(tok, tok * TOPK // experts_all + 2)
    fits = (
        tok <= ROWS
        and local_experts == 1
        and capacity <= SLOTS
        and d_model % (128 * n) == 0
        and n % n_tp == 0
        and n_tp == 2
        and experts_all <= 128
    )
    return fused(*args) if fits else on_device(*args)


def solution(mesh):
    return jax.shard_map(
        layer,
        mesh=mesh,
        in_specs=(
            P(("grp", "ep"), None),
            P(),
            P(),
            P("ep", "tp"),
            P("ep", "tp"),
            P("ep", "tp"),
            P("tp"),
            P(("grp", "ep"), None, "tp", None),
            P(("grp", "ep")),
            P("tp", "ep"),
            P(("grp", "ep"), None),
            P(("grp", "ep"), None),
            P("ep", None, "tp"),
            P("ep", None, "tp"),
            P("ep", "tp", None),
            P("ep", "tp"),
            P("ep", "tp"),
            P("tp", "ep"),
        ),
        out_specs=(P(("grp", "ep"), "tp"), P(("grp", "ep"), "tp", None)),
        check_vma=False,
    )
```

```python
import functools

import jax
import jax.numpy as jnp
from jax import lax
from jax.experimental import pallas as pl
from jax.experimental.pallas import tpu as pltpu
from jax.sharding import PartitionSpec as P

HEAD = 64
TOPK = 4


EPS = 1e-06


def rms_scale(row_block, gain):
    rows_wide = row_block.astype(jnp.float32)
    inverse = lax.rsqrt(jnp.mean(rows_wide * rows_wide, axis=-1, keepdims=True) + EPS)
    return rows_wide * inverse * gain


def stick_read(query, kv_cache, lengths, offsets):
    seq_count = query.shape[0]
    kv_local = kv_cache.shape[2]
    head_local = offsets.shape[0]
    per_group = head_local // kv_local
    cache_len = kv_cache.shape[1]
    grouped = query.reshape(seq_count, kv_local, per_group, HEAD)
    key_rows = kv_cache[:, :, :, :HEAD]
    value_rows = kv_cache[:, :, :, HEAD:]
    scores = jnp.einsum("skgd,slkd->skgl", grouped, key_rows, preferred_element_type=jnp.float32)
    scores = scores * HEAD ** (-0.5) - offsets.reshape(1, kv_local, per_group, 1)
    positions = lax.broadcasted_iota(jnp.int32, (seq_count, cache_len), 1)
    alive_mask = (positions < lengths[:, None])[:, None, None, :]
    remain = jnp.where(alive_mask, jax.nn.log_sigmoid(-scores), 0.0)
    suffix = lax.cumsum(remain, axis=3, reverse=True) - remain
    stick = jnp.where(alive_mask, jnp.exp(jax.nn.log_sigmoid(scores) + suffix), 0.0).astype(
        jnp.bfloat16
    )
    mixed_out = jnp.einsum("skgl,slkd->skgd", stick, value_rows, preferred_element_type=jnp.float32)
    return mixed_out.reshape(seq_count, head_local * HEAD).astype(jnp.bfloat16)


def on_device(
    resid_in,
    norm_attn,
    norm_moe,
    w_query,
    w_key,
    w_value,
    head_offset,
    kv_cache,
    lengths,
    w_output,
    routes,
    route_weights,
    gate_experts,
    up_experts,
    down_experts,
    gate_shared,
    up_shared,
    down_shared,
):
    tok_count = resid_in.shape[0]
    n_ep = lax.axis_size("ep")
    normed = rms_scale(resid_in, norm_attn).astype(jnp.bfloat16)
    k_cols = w_key.shape[1]
    pieces = (
        lax.all_gather(w_query, "ep", axis=0, tiled=True),
        lax.all_gather(w_key, "ep", axis=0, tiled=True),
        lax.all_gather(w_value, "ep", axis=0, tiled=True),
    )
    sliced = normed
    query_f, key_f, value_f = tuple(
        (
            jnp.dot(sliced, weight_piece, preferred_element_type=jnp.float32)
            for weight_piece in pieces
        )
    )
    query = query_f.astype(jnp.bfloat16)
    kv_local = k_cols // HEAD
    key_new = key_f.astype(jnp.bfloat16).reshape(tok_count, kv_local, HEAD)
    value_new = value_f.astype(jnp.bfloat16).reshape(tok_count, kv_local, HEAD)
    new_rows = jnp.concatenate([key_new, value_new], axis=2)
    attended = stick_read(query, kv_cache, lengths, head_offset)
    attn_part = jnp.dot(
        attended,
        lax.all_gather(w_output, "ep", axis=1, tiled=True),
        preferred_element_type=jnp.float32,
    ).astype(jnp.bfloat16)
    attn_sum = lax.psum(attn_part, "tp").astype(jnp.float32)
    resid_mid = (resid_in.astype(jnp.float32) + attn_sum).astype(jnp.bfloat16)
    normed_moe = rms_scale(resid_mid, norm_moe).astype(jnp.bfloat16)
    pieces = (
        lax.all_gather(gate_shared, "ep", axis=0, tiled=True),
        lax.all_gather(up_shared, "ep", axis=0, tiled=True),
    )
    sliced = normed_moe
    gate_s = jnp.dot(sliced, pieces[0], preferred_element_type=jnp.float32)
    up_s = jnp.dot(sliced, pieces[1], preferred_element_type=jnp.float32)
    hidden_shared = (jax.nn.silu(gate_s) * up_s).astype(jnp.bfloat16)
    shared_part = jnp.dot(
        hidden_shared,
        lax.all_gather(down_shared, "ep", axis=1, tiled=True),
        preferred_element_type=jnp.float32,
    ).astype(jnp.bfloat16)
    shared_out = lax.psum_scatter(shared_part, "tp", scatter_dimension=1, tiled=True).astype(
        jnp.float32
    )
    local_experts = gate_experts.shape[0]
    experts_all = local_experts * n_ep
    capacity = min(tok_count, tok_count * TOPK // experts_all + 2)
    flat_routes = routes.reshape(-1)
    expert_ids = lax.broadcasted_iota(jnp.int32, (1, experts_all), 1)
    onehot = (flat_routes[:, None] == expert_ids).astype(jnp.int32)
    slots = jnp.sum((jnp.cumsum(onehot, axis=0) - onehot) * onehot, axis=1)
    expert_grid = lax.broadcasted_iota(jnp.int32, (experts_all, capacity, 1), 0)
    slot_grid = lax.broadcasted_iota(jnp.int32, (experts_all, capacity, 1), 1)
    match = (
        (flat_routes[None, None, :] == expert_grid) & (slots[None, None, :] == slot_grid)
    ).astype(jnp.bfloat16)
    source_rows = jnp.repeat(normed_moe, TOPK, axis=0)
    outgoing = jnp.einsum(
        "ecr,rd->ecd", match, source_rows, preferred_element_type=jnp.float32
    ).astype(jnp.bfloat16)
    arrived = lax.all_to_all(outgoing, "ep", split_axis=0, concat_axis=0, tiled=True)
    slot_count = arrived.shape[1]
    grouped_in = arrived.reshape(n_ep, local_experts, slot_count, arrived.shape[2])
    gate_h = jnp.einsum(
        "secd,edf->secf", grouped_in, gate_experts, preferred_element_type=jnp.float32
    )
    up_h = jnp.einsum("secd,edf->secf", grouped_in, up_experts, preferred_element_type=jnp.float32)
    hidden_e = (jax.nn.silu(gate_h) * up_h).astype(jnp.bfloat16)
    down_h = jnp.einsum(
        "secf,efd->secd", hidden_e, down_experts, preferred_element_type=jnp.float32
    ).astype(jnp.bfloat16)
    summed = (
        lax.psum_scatter(down_h, "tp", scatter_dimension=3, tiled=True)
        .astype(jnp.float32)
        .astype(jnp.bfloat16)
    )
    summed = summed.reshape(n_ep * local_experts, slot_count, summed.shape[3])
    returned = lax.all_to_all(summed, "ep", split_axis=0, concat_axis=0, tiled=True)
    gathered_back = jnp.einsum("ecr,ecd->rd", match, returned, preferred_element_type=jnp.float32)
    col_width = gathered_back.shape[1]
    weighted = gathered_back.reshape(tok_count, TOPK, col_width) * route_weights[:, :, None]
    routed = jnp.sum(weighted, axis=1)
    own_cols = lax.dynamic_slice_in_dim(resid_mid, lax.axis_index("tp") * col_width, col_width, 1)
    layer_out = (own_cols.astype(jnp.float32) + shared_out + routed).astype(jnp.bfloat16)
    return (layer_out, new_rows)


MESH = pl.DeviceIdType.MESH
ROWS = 16
SLOTS = 8
BF = jnp.bfloat16
F32 = jnp.float32


def fdot(a, b):
    return jnp.dot(a, b, preferred_element_type=F32)


def iota(shape, dim):
    return lax.broadcasted_iota(jnp.int32, shape, dim)


def layer_kernel(
    n, n_tp, tok, resid_h, g_attn_h, g_moe_h, offs_h, lens_h, routes_h, rweights_h,
    wq_h, wk_h, wv_h, kv_h, wo_h, ge_h, ue_h, de_h, gs_h, us_h, ds_h,
    out_h, new_rows_h,
    resid, g_attn, g_moe, offs, lens, routes, rweights, out, new_rows, osem, wqkv, kv, wo, ge, ue, de, gus, dsh,
    x32, xs, xr, p2s, p2r, sc, st, oh, ags, agr, xps, xpr, dsp, dsr,
    s1s, s1r, hs, hr, fs, fr, f2s, f2r, rts, rws,
    lsem, s_p1, r_p1, s_p2, r_p2, s_ag, r_ag, s_x, r_x, s_d, r_d,
    s_s1, r_s1, s_s2, r_s2, s_f, r_f, s_f2, r_f2,
):
    me = lax.axis_index("ep")
    tp = lax.axis_index("tp")
    d_model = x32.shape[1]
    width = d_model // n
    qcols = wq_h.shape[1]
    kcols = wk_h.shape[1]
    heads = offs.shape[1]
    kv_local = kcols // HEAD
    per_group = heads // kv_local
    span = kv_h.shape[1]
    allrows = n * ROWS

    loads = []

    def load(src, dst):
        copy = pltpu.make_async_copy(src, dst, lsem.at[len(loads)])
        copy.start()
        loads.append(copy)
        return copy

    small = [
        load(resid_h, resid), load(routes_h, routes), load(rweights_h, rweights), load(g_attn_h, g_attn),
        load(g_moe_h, g_moe), load(offs_h, offs), load(lens_h, lens),
    ]
    l_qkv = [
        load(wq_h, wqkv.at[:, pl.ds(0, qcols)]),
        load(wk_h, wqkv.at[:, pl.ds(qcols, kcols)]),
        load(wv_h, wqkv.at[:, pl.ds(qcols + kcols, kcols)]),
    ]
    l_kv = [load(kv_h.at[s], kv.at[s]) for s in range(tok)]
    l_wo = load(wo_h, wo)
    fs_cols = gs_h.shape[1]
    l_gus = [load(gs_h, gus.at[:, pl.ds(0, fs_cols)]), load(us_h, gus.at[:, pl.ds(fs_cols, fs_cols)])]
    l_exp = [load(ge_h.at[0], ge), load(ue_h.at[0], ue), load(de_h.at[0], de)]
    l_ds = load(ds_h, dsh)

    barrier = pltpu.get_barrier_semaphore()
    for t in range(n_tp):
        for k in range(n):
            if t or k:
                pl.semaphore_signal(
                    barrier,
                    inc=1,
                    device_id={"ep": lax.rem(me + k, n), "tp": lax.rem(tp + t, n_tp)},
                    device_id_type=MESH,
                )

    for copy in small:
        copy.wait()
    x32[...] = jnp.zeros_like(x32)
    x32[0:tok, :] = resid[...].astype(F32)
    rts[...] = jnp.full(rts.shape, -1.0, F32)
    rts[:, 0:tok] = routes[...].astype(F32)
    rws[...] = jnp.zeros_like(rws)
    rws[:, 0:tok] = rweights[...]
    spot = (iota((TOPK, 128), 0) == iota((TOPK, 128), 1)).astype(F32)
    routes_rows = lax.dot_general(
        rts[...], spot, (((0,), (0,)), ((), ())), preferred_element_type=F32
    ).astype(BF)
    for j in range(n):
        xs[j, :, 0:width] = x32[:, j * width : (j + 1) * width].astype(BF)
        xs[j, :, width:] = routes_rows
    xr[me] = xs[me]

    pl.semaphore_wait(barrier, n * n_tp - 1)

    sent = []

    def exchange(src, dst, ssem, rsem):
        arrivals = []
        for k in range(1, n):
            peer = lax.rem(me + k, n)
            copy = pltpu.make_async_remote_copy(
                src_ref=src(peer), dst_ref=dst(me), send_sem=ssem.at[k], recv_sem=rsem.at[k],
                device_id={"ep": peer}, device_id_type=MESH,
            )
            copy.start()
            sent.append(copy)
            origin = lax.rem(me + n - k, n)
            arrivals.append(
                pltpu.make_async_remote_copy(
                    src_ref=src(peer), dst_ref=dst(origin), send_sem=ssem.at[k], recv_sem=rsem.at[k],
                    device_id={"ep": peer}, device_id_type=MESH,
                )
            )
        return arrivals

    def exchange_tp(t, src, dst, ssem, rsem):
        arrivals = []
        for k in range(n):
            if k or t:
                peer = lax.rem(me + k, n)
                peer_tp = lax.rem(tp + t, n_tp)
                origin = lax.rem(me + n - k, n)
                origin_tp = lax.rem(tp + n_tp - t, n_tp)
                i = t * n + k
                device = {"ep": peer, "tp": peer_tp}
                copy = pltpu.make_async_remote_copy(
                    src_ref=src(peer_tp, peer), dst_ref=dst(tp, me), send_sem=ssem.at[i],
                    recv_sem=rsem.at[i], device_id=device, device_id_type=MESH,
                )
                copy.start()
                sent.append(copy)
                arrivals.append(
                    pltpu.make_async_remote_copy(
                        src_ref=src(peer_tp, peer), dst_ref=dst(origin_tp, origin), send_sem=ssem.at[i],
                        recv_sem=rsem.at[i], device_id=device, device_id_type=MESH,
                    )
                )
        return arrivals

    def arrive(arrivals):
        for copy in arrivals:
            copy.wait_recv()

    got = exchange(lambda j: xs.at[j], lambda j: xr.at[j], s_p1, r_p1)
    inv_attn = lax.rsqrt(jnp.sum(x32[...] * x32[...], axis=1, keepdims=True) / d_model + EPS)
    for copy in l_qkv:
        copy.wait()
    arrive(got)
    gain_a = g_attn[:, pl.ds(pl.multiple_of(me * width, 128), width)]
    scaled = (xr[:, :, 0:width].reshape(allrows, width).astype(F32) * gain_a).astype(BF)
    p2s[...] = fdot(scaled, wqkv[...]).astype(BF).reshape(p2s.shape)
    p2r[me] = p2s[me]
    got = exchange(lambda j: p2s.at[j], lambda j: p2r.at[j], s_p2, r_p2)

    row = iota((tok * heads, 1), 0)
    head_of_row = lax.rem(row, heads)
    seq_of_row = row // heads
    off_col = jnp.sum(
        jnp.where(iota((tok * heads, heads), 1) == head_of_row, jnp.broadcast_to(offs[...], (tok * heads, heads)), 0.0),
        axis=1, keepdims=True,
    )
    len_col = jnp.sum(
        jnp.where(iota((tok * heads, tok), 1) == seq_of_row, jnp.broadcast_to(lens[...], (tok * heads, tok)).astype(F32), 0.0),
        axis=1, keepdims=True,
    )
    group_col = head_of_row // per_group
    fold = (lax.rem(iota((qcols, 2 * HEAD), 0), HEAD) == iota((qcols, 2 * HEAD), 1)).astype(F32).astype(BF)
    unfold = (lax.rem(iota((2 * HEAD, qcols), 1), HEAD) + HEAD == iota((2 * HEAD, qcols), 0)).astype(F32).astype(BF)
    head_mask = (iota((1, heads, qcols), 2) // HEAD == iota((1, heads, qcols), 1)).astype(F32)
    blk = 2 * 128
    later = (iota((blk, blk), 0) > iota((blk, blk), 1)).astype(F32).astype(BF)
    oh[...] = jnp.zeros_like(oh)

    arrive(got)
    qkv = jnp.sum(p2r[...].astype(F32), axis=0) * inv_attn
    q = qkv[:, :qcols].astype(BF).astype(F32)
    key = qkv[:, qcols : qcols + kcols]
    val = qkv[:, qcols + kcols :]
    parts = []
    for g in range(kv_local):
        parts += [key[:, g * HEAD : (g + 1) * HEAD], val[:, g * HEAD : (g + 1) * HEAD]]
    new_rows[...] = jnp.concatenate(parts, axis=1)[0:tok, :].astype(BF)
    put_rows = pltpu.make_async_copy(new_rows, new_rows_h, osem.at[0])
    put_rows.start()

    spread = (q[:, None, :] * head_mask).reshape(ROWS * heads, qcols).astype(BF)
    q8 = fdot(spread, fold) * HEAD ** (-0.5)
    for s in range(tok):
        l_kv[s].wait()
        sc[s * heads : (s + 1) * heads, :] = lax.dot_general(
            q8[s * heads : (s + 1) * heads, :].astype(BF), kv[s],
            (((1,), (1,)), ((), ())), preferred_element_type=F32,
        )
    carry = jnp.zeros((tok * heads, 1), F32)
    for b in reversed(range(span // blk)):
        x = sc[:, b * blk : (b + 1) * blk] - off_col
        where_to = iota((tok * heads, blk), 1) + b * blk
        alive = ((where_to // kv_local).astype(F32) < len_col) & (lax.rem(where_to, kv_local) == group_col)
        tail = jnp.log(1.0 + jnp.exp(-jnp.abs(x)))
        remain = jnp.where(alive, -(jnp.maximum(x, 0.0) + tail), 0.0)
        high = remain.astype(BF)
        low = (remain - high.astype(F32)).astype(BF)
        suffix = fdot(high, later) + fdot(low, later) + carry
        st[:, b * blk : (b + 1) * blk] = jnp.where(alive, jnp.exp(jnp.minimum(x, 0.0) - tail + suffix), 0.0)
        carry = carry + jnp.sum(remain, axis=1, keepdims=True)
    for s in range(tok):
        oh[s * heads : (s + 1) * heads, :] = fdot(st[s * heads : (s + 1) * heads, :].astype(BF), kv[s])
    wide = fdot(oh[...].astype(BF), unfold).reshape(ROWS, heads, qcols) * head_mask
    ags[...] = jnp.sum(wide, axis=1).astype(BF)
    agr[me] = ags[...]
    got = exchange(lambda j: ags, lambda j: agr.at[j], s_ag, r_ag)
    l_wo.wait()

    cgrid = iota((n * SLOTS, ROWS), 0)
    named = jnp.zeros((n * SLOTS, ROWS), F32)
    weight = jnp.zeros((n * SLOTS, ROWS), F32)
    for k in range(TOPK):
        hit = rts[k : k + 1, :] == (cgrid // SLOTS).astype(F32)
        named = named + jnp.where(hit, 1.0, 0.0)
        weight = weight + jnp.where(hit, jnp.broadcast_to(rws[k : k + 1, :], hit.shape), 0.0)
    before = (iota((ROWS, ROWS), 0) < iota((ROWS, ROWS), 1)).astype(F32).astype(BF)
    slot = fdot(named.astype(BF), before)
    pick = jnp.where(slot == lax.rem(cgrid, SLOTS).astype(F32), named, 0.0)
    weight = weight * pick
    per_expert = n * SLOTS
    all_routes = xr[:, :, width:].reshape(allrows, 128).astype(F32).T
    rgrid = iota((n * per_expert, allrows), 0)
    qgrid = iota((n * per_expert, allrows), 1)
    want = (rgrid // per_expert).astype(F32)
    named_all = jnp.zeros((n * per_expert, allrows), F32)
    for k in range(TOPK):
        named_all = named_all + jnp.where(all_routes[k : k + 1, :] == want, 1.0, 0.0)
    qa, qb = iota((allrows, allrows), 0), iota((allrows, allrows), 1)
    before_all = jnp.where((qa // ROWS == qb // ROWS) & (qa < qb), 1.0, 0.0).astype(BF)
    slot_all = fdot(named_all.astype(BF), before_all)
    right = (lax.rem(rgrid, per_expert) // SLOTS == qgrid // ROWS) & (
        slot_all == lax.rem(rgrid, SLOTS).astype(F32)
    )
    pick_all = jnp.where(right, named_all, 0.0).astype(BF)

    arrive(got)
    part = fdot(agr[...].reshape(allrows, qcols), wo[...]).astype(BF)
    xps[...] = part
    swap = pltpu.make_async_remote_copy(
        src_ref=xps, dst_ref=xpr, send_sem=s_x.at[0], recv_sem=r_x.at[0],
        device_id={"tp": lax.rem(tp + 1, n_tp)}, device_id_type=MESH,
    )
    swap.start()
    sent.append(swap)
    gain_m = g_moe[:, pl.ds(pl.multiple_of(me * width, 128), width)]
    base = xr[:, :, 0:width].reshape(allrows, width).astype(F32)
    for copy in l_gus:
        copy.wait()
    swap.wait_recv()
    mid = (base + (part.astype(F32) + xpr[...].astype(F32))).astype(BF)
    mid32 = mid.astype(F32)

    square = jnp.sum(mid32 * mid32, axis=1, keepdims=True)
    sq_high = square.astype(BF).astype(F32)
    lane = iota((allrows, 128), 1)
    sq_wide = jnp.where(lane == 0, sq_high, jnp.where(lane == 1, square - sq_high, 0.0))
    s1s[:, :, 0 : 2 * fs_cols] = fdot((mid32 * gain_m).astype(BF), gus[...]).astype(BF).reshape(n, ROWS, 2 * fs_cols)
    s1s[:, :, 2 * fs_cols :] = sq_wide.astype(BF).reshape(n, ROWS, 128)
    s1r[me] = s1s[me]
    got_s1 = exchange(lambda j: s1s.at[j], lambda j: s1r.at[j], s_s1, r_s1)
    dsp[...] = fdot(pick_all, mid).astype(BF).reshape(dsp.shape)
    dsr[me] = dsp[me]
    got_d = exchange(lambda j: dsp.at[j], lambda j: dsr.at[j], s_d, r_d)

    for copy in l_exp:
        copy.wait()
    l_ds.wait()
    arrive(got_s1)
    inv_own = lax.rsqrt(
        jnp.sum(jnp.sum(s1r[:, :, 2 * fs_cols :].astype(F32), axis=0), axis=1, keepdims=True) / d_model + EPS
    )
    both = jnp.sum(s1r[:, :, 0 : 2 * fs_cols].astype(F32), axis=0) * inv_own
    hs[...] = (jax.nn.silu(both[:, :fs_cols]) * both[:, fs_cols:]).astype(BF)
    hr[me] = hs[...]
    got_s2 = exchange(lambda j: hs, lambda j: hr.at[j], s_s2, r_s2)

    arrive(got_d)
    square = jnp.zeros((per_expert, 1), F32)
    for j in range(n):
        piece = dsr[j].astype(F32)
        square = square + jnp.sum(piece * piece, axis=1, keepdims=True)
    inv_moe = lax.rsqrt(square / d_model + EPS)
    rows_in = jnp.concatenate(
        [
            (dsr[j].astype(F32) * inv_moe * g_moe[:, j * width : (j + 1) * width]).astype(BF)
            for j in range(n)
        ],
        axis=1,
    )
    hidden = (jax.nn.silu(fdot(rows_in, ge[...])) * fdot(rows_in, ue[...])).astype(BF)
    half = d_model // n_tp
    got_f = []
    for t in reversed(range(n_tp)):
        to = lax.rem(tp + t, n_tp)
        cols = pl.ds(pl.multiple_of(to * half, 128), half)
        fs[to] = fdot(hidden, de[:, cols]).reshape(n, SLOTS, half).astype(BF)
        if t == 0:
            fr[tp, me] = fs[tp, me]
        got_f += exchange_tp(t, lambda t, j: fs.at[t, j], lambda t, j: fr.at[t, j], s_f, r_f)

    arrive(got_s2)
    chunks = n // n_tp
    target = me // chunks
    chunk = lax.rem(me, chunks)
    carried = jnp.where(tp == 0, 1.0, 0.0) * mid32
    f2s[...] = (fdot(hr[...].reshape(allrows, fs_cols), dsh[...]) + carried).astype(BF).reshape(f2s.shape)

    def give(k):
        peer = lax.rem(me + k, n)
        return pltpu.make_async_remote_copy(
            src_ref=f2s.at[peer], dst_ref=f2r.at[tp, chunk], send_sem=s_f2.at[k],
            recv_sem=r_f2.at[chunk * n_tp + tp], device_id={"ep": peer, "tp": target}, device_id_type=MESH,
        )

    for k in range(1, n):
        give(k).start()

    @pl.when(target != tp)
    def _():
        give(0).start()

    @pl.when(target == tp)
    def _():
        f2r[tp, chunk] = f2s[me]

    arrive(got_f)
    back = fr[0].astype(F32)
    for t in range(1, n_tp):
        back = back + fr[t].astype(F32)
    back = back.astype(BF).astype(F32).reshape(n * SLOTS, half)
    routed = lax.dot_general(
        weight, back, (((0,), (0,)), ((), ())), preferred_element_type=F32, precision=lax.Precision.HIGHEST
    )
    for c in range(chunks):
        for t in range(n_tp):

            @pl.when((tp * chunks + c != me) | (tp != t))
            def _():
                pltpu.make_async_remote_copy(
                    src_ref=f2s.at[me], dst_ref=f2r.at[t, c], send_sem=s_f2.at[0],
                    recv_sem=r_f2.at[c * n_tp + t], device_id={"tp": 1 - tp}, device_id_type=MESH,
                ).wait_recv()

    for c in range(chunks):
        total = routed[:, c * width : (c + 1) * width]
        for t in range(n_tp):
            total = total + f2r[t, c].astype(F32)
        out[:, c * width : (c + 1) * width] = total[0:tok, :].astype(BF)
    put_out = pltpu.make_async_copy(out, out_h, osem.at[1])
    put_out.start()
    for k in range(1, n):
        give(k).wait_send()

    @pl.when(target != tp)
    def _():
        give(0).wait_send()

    for copy in sent:
        copy.wait_send()
    put_rows.wait()
    put_out.wait()


def fused(
    resid_in, norm_attn, norm_moe, w_query, w_key, w_value, head_offset, kv_cache, lengths,
    w_output, routes, route_weights, gate_experts, up_experts, down_experts,
    gate_shared, up_shared, down_shared,
):
    n = lax.axis_size("ep")
    n_tp = lax.axis_size("tp")
    tok, d_model = resid_in.shape
    width = d_model // n
    qcols, kcols = w_query.shape[1], w_key.shape[1]
    heads = head_offset.shape[0]
    length, kv_local = kv_cache.shape[1:3]
    span = length * kv_local
    fe, fs_cols = gate_experts.shape[2], gate_shared.shape[1]
    half = d_model // n_tp
    qkv = qcols + 2 * kcols
    V = pltpu.VMEM
    dma = pltpu.SemaphoreType.DMA
    scratch = [
        V((tok, d_model), BF), V((1, d_model), F32), V((1, d_model), F32), V((1, heads), F32),
        V((1, tok), jnp.int32), V((TOPK, tok), jnp.int32), V((TOPK, tok), F32),
        V((tok, half), BF), V((tok, 2 * kcols), BF), dma((2,)),
        V((width, qkv), BF), V((tok, span, 2 * HEAD), BF), V(w_output.shape, BF),
        V((d_model, fe), BF), V((d_model, fe), BF), V((fe, d_model), BF),
        V((width, 2 * fs_cols), BF), V(down_shared.shape, BF),
        V((ROWS, d_model), F32), V((n, ROWS, width + 128), BF), V((n, ROWS, width + 128), BF),
        V((n, ROWS, qkv), BF), V((n, ROWS, qkv), BF),
        V((tok * heads, span), F32), V((tok * heads, span), F32), V((ROWS * heads, 2 * HEAD), F32),
        V((ROWS, qcols), BF), V((n, ROWS, qcols), BF),
        V((n * ROWS, width), BF), V((n * ROWS, width), BF),
        V((n, n * SLOTS, width), BF), V((n, n * SLOTS, width), BF),
        V((n, ROWS, 2 * fs_cols + 128), BF), V((n, ROWS, 2 * fs_cols + 128), BF),
        V((ROWS, fs_cols), BF), V((n, ROWS, fs_cols), BF),
        V((n_tp, n, SLOTS, half), BF), V((n_tp, n, SLOTS, half), BF),
        V((n, ROWS, width), BF), V((n_tp, n // n_tp, ROWS, width), BF),
        V((TOPK, ROWS), F32), V((TOPK, ROWS), F32),
        dma((17 + tok,)),
    ]
    scratch += [dma((n,))] * 6 + [dma((1,))] * 2 + [dma((n,))] * 6 + [dma((n_tp * n,))] * 2 + [dma((n,))] * 2
    in_hbm = pl.BlockSpec(memory_space=pl.ANY)
    out, rows = pl.pallas_call(
        functools.partial(layer_kernel, n, n_tp, tok),
        out_shape=(
            jax.ShapeDtypeStruct((tok, half), BF),
            jax.ShapeDtypeStruct((tok, 2 * kcols), BF),
        ),
        in_specs=[in_hbm] * 18,
        out_specs=(in_hbm, in_hbm),
        scratch_shapes=scratch,
        compiler_params=pltpu.CompilerParams(
            collective_id=0, has_side_effects=True, vmem_limit_bytes=60 * 2**20
        ),
    )(
        resid_in, norm_attn.reshape(1, -1), norm_moe.reshape(1, -1), head_offset.reshape(1, -1),
        lengths.reshape(1, -1), routes.T, route_weights.T,
        w_query, w_key, w_value, kv_cache.reshape(tok, span, 2 * HEAD), w_output,
        gate_experts, up_experts, down_experts, gate_shared, up_shared, down_shared,
    )
    return out, rows.reshape(tok, kv_local, 2 * HEAD)


def layer(*args):
    n = lax.axis_size("ep")
    n_tp = lax.axis_size("tp")
    tok, d_model = args[0].shape
    local_experts = args[12].shape[0]
    experts_all = local_experts * n
    capacity = min(tok, tok * TOPK // experts_all + 2)
    fits = (
        tok <= ROWS
        and local_experts == 1
        and capacity <= SLOTS
        and d_model % (128 * n) == 0
        and n % n_tp == 0
        and n_tp == 2
        and experts_all <= 128
    )
    return fused(*args) if fits else on_device(*args)


def solution(mesh):
    return jax.shard_map(
        layer,
        mesh=mesh,
        in_specs=(
            P(("grp", "ep"), None),
            P(),
            P(),
            P("ep", "tp"),
            P("ep", "tp"),
            P("ep", "tp"),
            P("tp"),
            P(("grp", "ep"), None, "tp", None),
            P(("grp", "ep")),
            P("tp", "ep"),
            P(("grp", "ep"), None),
            P(("grp", "ep"), None),
            P("ep", None, "tp"),
            P("ep", None, "tp"),
            P("ep", "tp", None),
            P("ep", "tp"),
            P("ep", "tp"),
            P("tp", "ep"),
        ),
        out_specs=(P(("grp", "ep"), "tp"), P(("grp", "ep"), "tp", None)),
        check_vma=False,
    )
```
